32 devices in a mesh: row: 8 (over z, x), col: 4 (over y, core).
Axes of the slice: x: 2, y: 2, z: 4, core: 2. Of those that a mesh axis runs over, the one named last changes fastest.
Arguments:
- tokens: bfloat16 [16384, 4096], P(('row', 'col')), may hold values from -36 to 36
- norm_gain: bfloat16 [4096], replicated, may hold values from 0.099609375 to 1.8984375
- in_weight: bfloat16 [4096, 1024], replicated, may hold values from -0.09375 to 0.09375
- out_weight: bfloat16 [1024, 4096], replicated, may hold values from -0.1875 to 0.1875
Outputs:
- mixed: bfloat16 [16384, 4096], P(('row', 'col'))
The draws below stay inside these ranges and needn't reach their ends.
All inputs are finite; a program needn't handle non-finite values.
Results may differ from the reference program's by a relative error of at most 0.0071.
Values may be sent and summed in bfloat16 or wider, within the bound.
A program may use at most 128 MiB of HBM per device.

```python
import jax
import jax.numpy as jnp
from jax import lax

D = 4096
GROUP_WIDTH = 64
F = 1024
TOKENS = 16384


def draw_tokens(key, part):
    keys = jax.random.split(key, 3)
    base = jnp.clip(jax.random.normal(keys[0], (TOKENS, D), jnp.float32), -4.0, 4.0)
    row_scales = jnp.exp(jax.random.uniform(keys[1], (TOKENS, 1), jnp.float32, -1.2, 1.0986))
    col_scales = jnp.exp(jax.random.uniform(keys[2], (1, D), jnp.float32, -1.2, 1.0986))
    return (base * row_scales * col_scales).astype(jnp.bfloat16)


def scatter_about(rng, extent, spread, limit, held_as=jnp.bfloat16):
    return jnp.clip(spread * jax.random.normal(rng, extent, jnp.float32), -limit, limit).astype(held_as)


def setup_inputs(seed: int = 0) -> dict:
    streams_of = jax.random.split(jax.random.key(seed), 5)
    return {
        "tokens": draw_tokens(jax.random.fold_in(streams_of[4], 71), 0),
        "norm_gain": jnp.clip(1.0 + 0.18 * jax.random.normal(streams_of[1], (D,), jnp.float32), 0.099609375, 1.8984375).astype(jnp.bfloat16),
        "in_weight": scatter_about(streams_of[2], (D, F), D ** -0.5, 0.09375),
        "out_weight": scatter_about(streams_of[3], (F, D), F ** -0.5, 0.1875),
    }


def reference(tokens, norm_gain, in_weight, out_weight):
    floats = tokens.astype(jnp.float32)
    scaling = lax.rsqrt(lax.optimization_barrier(jnp.mean(floats * floats, axis=-1, keepdims=True)) + 1e-06)
    normed = (floats * scaling * norm_gain.astype(jnp.float32)).astype(jnp.bfloat16)
    hidden = jnp.dot(normed, in_weight, preferred_element_type=jnp.float32).astype(jnp.bfloat16)
    widened = lax.optimization_barrier(hidden).astype(jnp.float32)
    length = widened.shape[0]
    grouped = widened.reshape(length, widened.shape[1] // GROUP_WIDTH, GROUP_WIDTH)
    channel_spectrum = jnp.fft.fft(grouped, axis=2, norm='ortho')
    real_rounded = channel_spectrum.real.astype(jnp.bfloat16)
    imag_rounded = channel_spectrum.imag.astype(jnp.bfloat16)
    real_rounded, imag_rounded = lax.optimization_barrier((real_rounded, imag_rounded))
    combined = real_rounded.astype(jnp.float32) + 1j * imag_rounded.astype(jnp.float32)
    spectrum = jnp.fft.fft(combined, axis=0, norm='ortho').real
    spectrum = spectrum.reshape(length, widened.shape[1]).astype(jnp.bfloat16)
    return jnp.dot(spectrum, out_weight, preferred_element_type=jnp.float32).astype(jnp.bfloat16)
```

```python
import functools
import math

import jax
import jax.numpy as jnp
import numpy as np
from jax import lax
from jax.experimental import pallas as pl
from jax.experimental.pallas import tpu as pltpu
from jax.sharding import PartitionSpec as P

GROUP_WIDTH = 64
AXES = ("row", "col")


def channel_tables(slots):
    pairs = slots // 2
    half = GROUP_WIDTH // 2
    index = np.arange(GROUP_WIDTH)
    forward = np.zeros((GROUP_WIDTH, GROUP_WIDTH))
    order = np.zeros((GROUP_WIDTH, GROUP_WIDTH))
    for slot in range(GROUP_WIDTH):
        place, within = divmod(slot, slots)
        pair = place * pairs + within % pairs
        angles = 2.0 * math.pi / GROUP_WIDTH * (pair * index % GROUP_WIDTH)
        if within < pairs:
            forward[slot] = np.cos(angles)
            order[pair, slot] = 1.0
        elif pair == 0:
            forward[slot] = np.cos(math.pi * index)
            order[half, slot] = 1.0
        else:
            forward[slot] = np.sin(angles)
            order[GROUP_WIDTH - pair, slot] = 1.0
    forward /= math.sqrt(GROUP_WIDTH)
    return forward.astype(jnp.bfloat16), order.astype(jnp.bfloat16)


def position_tables(outer, inner, devices):
    length = outer * inner
    k1 = np.arange(outer)
    n2 = np.arange(inner)
    n1_order = k1.reshape(devices, -1).T.reshape(-1)
    k2_order = n2.reshape(devices, -1).T.reshape(-1)
    one = 2.0 * math.pi / outer * (np.outer(n1_order, k1) % outer)
    first = np.concatenate([np.cos(one), -np.sin(one)], axis=1)
    turn = 2.0 * math.pi / length * np.outer(n2, k1)
    two = 2.0 * math.pi / inner * (np.outer(k2_order, n2) % inner)
    scale = 1.0 / math.sqrt(length)
    c, s, z = np.cos(two) * scale, np.sin(two) * scale, np.zeros((inner, inner))
    usual = np.block([[c, s, -s, c], [c, s, s, -c]])
    zeroth = np.block([[c, s, z, z], [z, z, c, s]])
    return (
        first.astype(jnp.bfloat16),
        np.cos(turn).astype(np.float32),
        np.sin(turn).astype(np.float32),
        usual.astype(jnp.bfloat16),
        zeroth.astype(jnp.bfloat16),
    )


PLANES = 4
HALVES = 2
LANES = 128
MESH = pl.DeviceIdType.MESH


def place_of(device, columns):
    return (device // columns, device % columns)


def turned_plane(plane, step):
    high = (plane // 2 + 1 - step // 2) % 2
    low = (plane % 2 + (step + 1) // 2) % 2
    return 2 * high + low


def here(devices):
    columns = lax.axis_size("col")
    me = lax.axis_index("row") * columns + lax.axis_index("col")
    per = devices // PLANES
    return me, columns, per, me // per, me % per


def greet(devices):
    me, columns, _, _, _ = here(devices)
    barrier = pltpu.get_barrier_semaphore()

    def signal(step, carry):
        other = (me + step) % devices
        pl.semaphore_signal(barrier, inc=1, device_id=place_of(other, columns), device_id_type=MESH)
        return carry

    lax.fori_loop(1, devices, signal, 0)
    return lambda: pl.semaphore_wait(barrier, devices - 1)


def send_plane(devices, step, from_ref, to_ref, send_sem, recv_sem, first):
    me, columns, per, plane, lane = here(devices)
    target_plane = turned_plane(plane, step)

    def send(hop, carry):
        target = target_plane * per + (lane + hop) % per
        pltpu.make_async_remote_copy(
            src_ref=from_ref.at[target],
            dst_ref=to_ref.at[me],
            send_sem=send_sem,
            recv_sem=recv_sem,
            device_id=place_of(target, columns),
            device_id_type=MESH,
        ).start()
        return carry

    lax.fori_loop(first, per, send, 0)


def wait_for(ref, sem, count):
    part = ref.at[pl.ds(0, count)]
    pltpu.make_async_copy(part, part, sem).wait()


def mixer_kernel(
    devices,
    tokens,
    weight,
    out_weight,
    gain_hbm,
    forward_hbm,
    first_hbm,
    turn_cos_hbm,
    turn_sin_hbm,
    usual_hbm,
    special_hbm,
    order_hbm,
    total,
    last,
    last_weight,
    gain,
    forward,
    first,
    turn_cos,
    turn_sin,
    usual,
    special,
    order,
    raw,
    held,
    held_out,
    wide,
    squares,
    sent,
    taken,
    table,
    grid,
    done,
    back,
    landed,
    ordered,
    token_sem,
    weight_sem,
    out_sem,
    last_sem,
    own_sem,
    send_sem,
    recv_sem,
    own_back_sem,
    back_sem,
    landed_sem,
    table_sem,
):
    me, columns, per, plane, lane = here(devices)
    pieces = token_sem.shape[0]
    rows, depth = raw.shape
    piece = rows // pieces
    width = held.shape[2]
    units, _, slots, _ = sent.shape
    members = devices // HALVES
    near = plane // HALVES
    far = (near + 1) % HALVES
    pairs = slots // 2
    places = GROUP_WIDTH // slots
    outer = first.shape[0]
    inner = turn_cos.shape[0]
    chunks = units * HALVES

    def token_copy(index):
        part = pl.ds(index * piece, piece)
        return pltpu.make_async_copy(tokens.at[part], raw.at[part], token_sem.at[index])

    def half_of(number):
        return (near + 1 + number) % HALVES

    def weight_copy(step):
        begin = pl.multiple_of((step // HALVES * HALVES + half_of(step % HALVES)) * width, width)
        return pltpu.make_async_copy(weight.at[:, pl.ds(begin, width)], held.at[step], weight_sem.at[step])

    out_width = out_weight.shape[1]
    far_begin = pl.multiple_of(((units - 1) * HALVES + far) * width, width)
    out_copy = pltpu.make_async_copy(out_weight, held_out, out_sem)
    last_copy = pltpu.make_async_copy(out_weight.at[pl.ds(far_begin, width)], last_weight, last_sem)

    distant = (gain_hbm, forward_hbm, first_hbm, turn_cos_hbm, turn_sin_hbm, usual_hbm, special_hbm, order_hbm)
    nearby = (gain, forward, first, turn_cos, turn_sin, usual, special, order)
    table_copies = [
        pltpu.make_async_copy(a, b, table_sem.at[index]) for index, (a, b) in enumerate(zip(distant, nearby))
    ]
    table_copies[0].start()
    for index in range(pieces):
        token_copy(index).start()
    weight_copy(0).start()
    table_copies[1].start()
    arrive = greet(devices)

    block = wide.shape[0]
    table_copies[0].wait()
    wide[...] = jnp.broadcast_to(gain[...].astype(jnp.float32).reshape(1, depth), wide.shape).astype(jnp.bfloat16)
    for index in range(pieces):
        token_copy(index).wait()

        def gather_squares(number, carry):
            part = pl.ds(pl.multiple_of(index * piece + number * block, block), block)
            parts = [jnp.zeros((block, LANES), jnp.float32) for _ in range(4)]
            for column in range(depth // LANES):
                across = pl.ds(column * LANES, LANES)
                values = raw[part, across]
                floats = values.astype(jnp.float32)
                parts[column % 4] = parts[column % 4] + floats * floats
                raw[part, across] = values * wide[:, across]
            squares[part, :] = (parts[0] + parts[1]) + (parts[2] + parts[3])
            return carry

        lax.fori_loop(0, piece // block, gather_squares, 0)
    for step in range(1, chunks):
        weight_copy(step).start()
    for copy in table_copies[2:]:
        copy.start()
    table_copies[1].wait()
    mean = jnp.sum(squares[...], axis=-1, keepdims=True) * (1.0 / depth)
    squares[...] = jnp.broadcast_to(lax.rsqrt(mean + 1e-06), squares.shape)

    arrive()

    def chunk(step, carry):
        unit = step // HALVES
        number = step % HALVES
        half = half_of(number)
        weight_copy(step).wait()
        product = jnp.dot(raw[...], held[step], preferred_element_type=jnp.float32)
        scaling = jnp.concatenate([squares[...]] * (width // LANES), axis=1)
        hidden = (product * scaling).astype(jnp.bfloat16)
        spectrum = lax.dot_general(
            forward[...], hidden, (((1,), (1,)), ((), ())), preferred_element_type=jnp.float32
        )
        sent[unit, pl.ds(half * members, members)] = spectrum.reshape(members, slots, rows).astype(jnp.bfloat16)
        for inside in range(PLANES // HALVES):
            plane_step = number * (PLANES // HALVES) + inside
            send_plane(
                devices,
                plane_step,
                sent.at[unit],
                taken.at[unit],
                send_sem.at[unit],
                recv_sem.at[unit],
                plane_step // (PLANES - 1),
            )
        return carry

    lax.fori_loop(0, chunks, chunk, 0)
    for unit in range(units):
        pltpu.make_async_copy(sent.at[unit, me], taken.at[unit, me], own_sem.at[unit]).start()
    out_copy.start()
    last_copy.start()

    for copy in table_copies[2:]:
        copy.wait()
    zeroth_here = me % places == 0

    @pl.when(zeroth_here)
    def _():
        table[...] = special[...]

    @pl.when(jnp.logical_not(zeroth_here))
    def _():
        table[...] = usual[...]

    def turned(slot):
        a = lax.dot_general(
            grid[slot], first[...], (((0,), (0,)), ((), ())), preferred_element_type=jnp.float32
        )
        re, im = a[:, :outer], a[:, outer:]
        c, s = turn_cos[...], turn_sin[...]
        return [(re * c + im * s).astype(jnp.bfloat16), (im * c - re * s).astype(jnp.bfloat16)]

    for unit in range(units):
        pltpu.make_async_copy(sent.at[unit, me], taken.at[unit, me], own_sem.at[unit]).wait()
        wait_for(taken.at[unit], recv_sem.at[unit], devices - 1)
        for part in range(outer // devices):
            piece_of = taken[unit, :, :, part * inner : (part + 1) * inner]
            grid[:, part * devices : (part + 1) * devices, :] = jnp.swapaxes(
                piece_of.astype(jnp.float32), 0, 1
            ).astype(jnp.bfloat16)
        for pair in range(pairs):
            b = jnp.concatenate(turned(pair) + turned(pair + pairs), axis=0)
            here_table = table if pair == 0 else usual
            o = jnp.dot(here_table[...], b, preferred_element_type=jnp.float32)
            done[pair] = o[:inner]
            done[pair + pairs] = o[inner:]
        for part in range(inner // devices):
            piece_of = done[:, part * devices : (part + 1) * devices, :]
            back[unit, :, :, part * outer : (part + 1) * outer] = jnp.swapaxes(piece_of, 0, 1).astype(jnp.bfloat16)
        for step in range(PLANES):
            send_plane(
                devices,
                step,
                back.at[unit],
                landed.at[unit],
                back_sem.at[unit],
                landed_sem.at[unit, step // HALVES],
                step // (PLANES - 1),
            )
        pltpu.make_async_copy(back.at[unit, me], landed.at[unit, me], own_back_sem.at[unit]).start()

    def put_in_order(unit, half):
        parts = landed[unit, pl.ds(half * members, members)].astype(jnp.float32)
        joined = parts.reshape(width, rows).astype(jnp.bfloat16)
        return lax.dot_general(
            joined, order[...], (((0,), (0,)), ((), ())), preferred_element_type=jnp.float32
        ).astype(jnp.bfloat16)

    tile = out_width // 8
    out_copy.wait()
    for unit in range(units):
        pltpu.make_async_copy(back.at[unit, me], landed.at[unit, me], own_back_sem.at[unit]).wait()
        for number in reversed(range(HALVES)):
            wait_for(landed.at[unit], landed_sem.at[unit, number], members - number)
            half = half_of(number)
            if unit == units - 1 and number == 0:
                last[...] = put_in_order(unit, half)
                continue
            ordered[...] = put_in_order(unit, half)
            begin = pl.multiple_of((unit * HALVES + half) * width, width)
            starting = unit == 0 and number == HALVES - 1

            def add_up(index, carry):
                across = pl.ds(pl.multiple_of(index * tile, tile), tile)
                product = jnp.dot(
                    ordered[...], held_out[pl.ds(begin, width), across], preferred_element_type=jnp.float32
                )
                total[:, across] = product if starting else total[:, across] + product
                return carry

            lax.fori_loop(0, out_width // tile, add_up, 0)

    last_copy.wait()
    for unit in range(units):
        wait_for(sent.at[unit], send_sem.at[unit], devices - 1)
        wait_for(back.at[unit], back_sem.at[unit], devices - 1)


def mixer(tokens, gain, weight, out_weight, forward, tables, order, units, devices):
    rows, depth = tokens.shape
    channels = weight.shape[1]
    slots = channels // devices // units
    outer = tables[0].shape[0]
    inner = tables[1].shape[0]
    width = channels // units // HALVES
    out_width = out_weight.shape[1]
    whole = pl.BlockSpec(memory_space=pltpu.VMEM)
    hbm = pl.BlockSpec(memory_space=pltpu.HBM)
    pieces = 4
    block = 16
    small = (gain, forward, *tables, order)
    return pl.pallas_call(
        functools.partial(mixer_kernel, devices),
        out_shape=(
            pltpu.VMEM((rows, out_width), jnp.float32),
            pltpu.VMEM((rows, width), jnp.bfloat16),
            pltpu.VMEM((width, out_width), jnp.bfloat16),
        ),
        in_specs=[hbm] * (3 + len(small)),
        out_specs=(whole, whole, whole),
        scratch_shapes=[pltpu.VMEM(table.shape, table.dtype) for table in small] + [
            pltpu.VMEM((rows, depth), jnp.bfloat16),
            pltpu.VMEM((units * HALVES, depth, width), jnp.bfloat16),
            pltpu.VMEM((channels, out_width), jnp.bfloat16),
            pltpu.VMEM((block, depth), jnp.bfloat16),
            pltpu.VMEM((rows, LANES), jnp.float32),
            pltpu.VMEM((units, devices, slots, rows), jnp.bfloat16),
            pltpu.VMEM((units, devices, slots, rows), jnp.bfloat16),
            pltpu.VMEM(tables[3].shape, jnp.bfloat16),
            pltpu.VMEM((slots, outer, inner), jnp.bfloat16),
            pltpu.VMEM((slots, inner, outer), jnp.float32),
            pltpu.VMEM((units, devices, slots, rows), jnp.bfloat16),
            pltpu.VMEM((units, devices, slots, rows), jnp.bfloat16),
            pltpu.VMEM((rows, width), jnp.bfloat16),
            pltpu.SemaphoreType.DMA((pieces,)),
            pltpu.SemaphoreType.DMA((units * HALVES,)),
            pltpu.SemaphoreType.DMA,
            pltpu.SemaphoreType.DMA,
            pltpu.SemaphoreType.DMA((units,)),
            pltpu.SemaphoreType.DMA((units,)),
            pltpu.SemaphoreType.DMA((units,)),
            pltpu.SemaphoreType.DMA((units,)),
            pltpu.SemaphoreType.DMA((units,)),
            pltpu.SemaphoreType.DMA((units, HALVES)),
            pltpu.SemaphoreType.DMA((len(small),)),
        ],
        compiler_params=pltpu.CompilerParams(collective_id=0, has_side_effects=True, vmem_limit_bytes=46 << 20),
    )(*[pltpu.with_memory_space_constraint(array, pltpu.HBM) for array in (tokens, weight, out_weight, *small)])


def local(tokens, norm_gain, in_weight, out_weight):
    rows_here = tokens.shape[0]
    channels = in_weight.shape[1]
    devices = lax.axis_size(AXES)
    slots = channels // devices
    units = max(1, slots // 16)
    length = rows_here * devices
    inner = 1 << ((length.bit_length()) // 2)
    outer = length // inner

    forward, order = channel_tables(slots // units)
    several = np.eye(channels // units // HALVES // GROUP_WIDTH)
    forward = np.kron(several, forward.astype(np.float32)).astype(jnp.bfloat16)
    order = np.kron(several, order.astype(np.float32)).T.astype(jnp.bfloat16)
    tables = position_tables(outer, inner, devices)
    total, last, last_weight = mixer(
        tokens, norm_gain, in_weight, out_weight, forward, tables, order, units, devices
    )
    return (total + jnp.dot(last, last_weight, preferred_element_type=jnp.float32)).astype(jnp.bfloat16)


def solution(mesh):
    placed = (P(AXES, None), P(), P(), P())
    return jax.shard_map(
        local, mesh=mesh, in_specs=placed, out_specs=P(AXES, None), check_vma=False
    )
```

```python
import functools
import math

import jax
import jax.numpy as jnp
import numpy as np
from jax import lax
from jax.experimental import pallas as pl
from jax.experimental.pallas import tpu as pltpu
from jax.sharding import PartitionSpec as P

GROUP_WIDTH = 64
AXES = ("row", "col")


def channel_tables(slots):
    pairs = slots // 2
    half = GROUP_WIDTH // 2
    index = np.arange(GROUP_WIDTH)
    forward = np.zeros((GROUP_WIDTH, GROUP_WIDTH))
    order = np.zeros((GROUP_WIDTH, GROUP_WIDTH))
    for slot in range(GROUP_WIDTH):
        place, within = divmod(slot, slots)
        pair = place * pairs + within % pairs
        angles = 2.0 * math.pi / GROUP_WIDTH * (pair * index % GROUP_WIDTH)
        if within < pairs:
            forward[slot] = np.cos(angles)
            order[pair, slot] = 1.0
        elif pair == 0:
            forward[slot] = np.cos(math.pi * index)
            order[half, slot] = 1.0
        else:
            forward[slot] = np.sin(angles)
            order[GROUP_WIDTH - pair, slot] = 1.0
    forward /= math.sqrt(GROUP_WIDTH)
    return forward.astype(jnp.bfloat16), order.astype(jnp.bfloat16)


def position_tables(outer, inner, devices):
    length = outer * inner
    k1 = np.arange(outer)
    n2 = np.arange(inner)
    n1_order = k1.reshape(devices, -1).T.reshape(-1)
    k2_order = n2.reshape(devices, -1).T.reshape(-1)
    one = 2.0 * math.pi / outer * (np.outer(n1_order, k1) % outer)
    first = np.concatenate([np.cos(one), -np.sin(one)], axis=1)
    turn = 2.0 * math.pi / length * np.outer(n2, k1)
    two = 2.0 * math.pi / inner * (np.outer(k2_order, n2) % inner)
    scale = 1.0 / math.sqrt(length)
    c, s, z = np.cos(two) * scale, np.sin(two) * scale, np.zeros((inner, inner))
    usual = np.block([[c, s, -s, c], [c, s, s, -c]])
    zeroth = np.block([[c, s, z, z], [z, z, c, s]])
    return (
        first.astype(jnp.bfloat16),
        np.cos(turn).astype(np.float32),
        np.sin(turn).astype(np.float32),
        usual.astype(jnp.bfloat16),
        zeroth.astype(jnp.bfloat16),
    )


PLANES = 4
HALVES = 2
SPLIT = 2
LANES = 128
MESH = pl.DeviceIdType.MESH


def place_of(device, columns):
    return (device // columns, device % columns)


def turned_plane(plane, step):
    high = (plane // 2 + 1 - step // 2) % 2
    low = (plane % 2 + (step + 1) // 2) % 2
    return 2 * high + low


def here(devices):
    columns = lax.axis_size("col")
    me = lax.axis_index("row") * columns + lax.axis_index("col")
    per = devices // PLANES
    return me, columns, per, me // per, me % per


def greet(devices):
    me, columns, _, _, _ = here(devices)
    barrier = pltpu.get_barrier_semaphore()

    def signal(step, carry):
        other = (me + step) % devices
        pl.semaphore_signal(barrier, inc=1, device_id=place_of(other, columns), device_id_type=MESH)
        return carry

    lax.fori_loop(1, devices, signal, 0)
    return lambda: pl.semaphore_wait(barrier, devices - 1)


def send_plane(devices, step, from_ref, to_ref, send_sem, recv_sem, first, across=slice(None)):
    me, columns, per, plane, lane = here(devices)
    target_plane = turned_plane(plane, step)

    def send(hop, carry):
        target = target_plane * per + (lane + hop) % per
        pltpu.make_async_remote_copy(
            src_ref=from_ref.at[target, :, across],
            dst_ref=to_ref.at[me, :, across],
            send_sem=send_sem,
            recv_sem=recv_sem,
            device_id=place_of(target, columns),
            device_id_type=MESH,
        ).start()
        return carry

    lax.fori_loop(first, per, send, 0)


def wait_for(ref, sem, count):
    part = ref.at[pl.ds(0, count)]
    pltpu.make_async_copy(part, part, sem).wait()


def mixer_kernel(
    devices,
    tokens,
    weight,
    out_weight,
    gain_hbm,
    forward_hbm,
    first_hbm,
    turn_cos_hbm,
    turn_sin_hbm,
    usual_hbm,
    special_hbm,
    order_hbm,
    total,
    last,
    last_weight,
    gain,
    forward,
    first,
    turn_cos,
    turn_sin,
    usual,
    special,
    order,
    raw,
    held,
    held_out,
    wide,
    squares,
    sent,
    taken,
    table,
    grid,
    done,
    back,
    landed,
    ordered,
    token_sem,
    first_weight_sem,
    weight_sem,
    out_sem,
    last_sem,
    own_sem,
    send_sem,
    recv_sem,
    own_back_sem,
    back_sem,
    landed_sem,
    table_sem,
):
    me, columns, per, plane, lane = here(devices)
    pieces = token_sem.shape[0]
    rows, depth = raw.shape
    piece = rows // pieces
    first_piece = depth // pieces
    width = held.shape[2]
    units, _, slots, _ = sent.shape
    members = devices // HALVES
    near = plane // HALVES
    far = (near + 1) % HALVES
    pairs = slots // 2
    places = GROUP_WIDTH // slots
    outer = first.shape[0]
    inner = turn_cos.shape[0]
    chunks = units * HALVES

    def token_copy(index):
        part = pl.ds(index * piece, piece)
        return pltpu.make_async_copy(tokens.at[part], raw.at[part], token_sem.at[index])

    def half_of(number):
        return (near + 1 + number) % HALVES

    def weight_copy(step):
        begin = pl.multiple_of((step // HALVES * HALVES + half_of(step % HALVES)) * width, width)
        return pltpu.make_async_copy(weight.at[:, pl.ds(begin, width)], held.at[step], weight_sem.at[step])

    def first_weight_copy(index):
        part = pl.ds(index * first_piece, first_piece)
        begin = pl.multiple_of(half_of(0) * width, width)
        return pltpu.make_async_copy(
            weight.at[part, pl.ds(begin, width)], held.at[0, part], first_weight_sem.at[index]
        )

    out_width = out_weight.shape[1]
    far_begin = pl.multiple_of(((units - 1) * HALVES + far) * width, width)
    out_copy = pltpu.make_async_copy(out_weight, held_out, out_sem)
    last_copy = pltpu.make_async_copy(out_weight.at[pl.ds(far_begin, width)], last_weight, last_sem)

    distant = (gain_hbm, forward_hbm, first_hbm, turn_cos_hbm, turn_sin_hbm, usual_hbm, special_hbm, order_hbm)
    nearby = (gain, forward, first, turn_cos, turn_sin, usual, special, order)
    table_copies = [
        pltpu.make_async_copy(a, b, table_sem.at[index]) for index, (a, b) in enumerate(zip(distant, nearby))
    ]
    table_copies[0].start()
    ahead = pieces // SPLIT
    for index in range(ahead):
        token_copy(index).start()
    for index in range(pieces):
        first_weight_copy(index).start()
    table_copies[1].start()
    arrive = greet(devices)

    block = wide.shape[0]
    table_copies[0].wait()
    wide[...] = jnp.broadcast_to(gain[...].astype(jnp.float32).reshape(1, depth), wide.shape).astype(jnp.bfloat16)

    def give_out(unit, number, part, product):
        half = half_of(number)
        scaling = jnp.concatenate([squares[part, :]] * (width // LANES), axis=1)
        hidden = (product * scaling).astype(jnp.bfloat16)
        spectrum = lax.dot_general(
            forward[...], hidden, (((1,), (1,)), ((), ())), preferred_element_type=jnp.float32
        )
        sent[unit, pl.ds(half * members, members), :, part] = spectrum.reshape(
            members, slots, part.size
        ).astype(jnp.bfloat16)

    def send_out(unit, number, part):
        for inside in range(PLANES // HALVES):
            plane_step = number * (PLANES // HALVES) + inside
            send_plane(
                devices,
                plane_step,
                sent.at[unit],
                taken.at[unit],
                send_sem.at[unit],
                recv_sem.at[unit],
                plane_step // (PLANES - 1),
                part,
            )

    def gather_squares(number, carry):
        part = pl.ds(pl.multiple_of(number * block, block), block)
        parts = [jnp.zeros((block, LANES), jnp.float32) for _ in range(4)]
        for column in range(depth // LANES):
            across = pl.ds(column * LANES, LANES)
            values = raw[part, across]
            floats = values.astype(jnp.float32)
            parts[column % 4] = parts[column % 4] + floats * floats
            raw[part, across] = values * wide[:, across]
        squares[part, :] = (parts[0] + parts[1]) + (parts[2] + parts[3])
        return carry

    begun = rows // SPLIT
    for stage in range(SPLIT):
        part = pl.ds(stage * begun, begun)
        for index in range(stage * ahead, (stage + 1) * ahead):
            token_copy(index).wait()
            if stage < SPLIT - 1:
                token_copy(index + ahead).start()
            lax.fori_loop(index * piece // block, (index + 1) * piece // block, gather_squares, 0)
        mean = jnp.sum(squares[part, :], axis=-1, keepdims=True) * (1.0 / depth)
        squares[part, :] = jnp.broadcast_to(lax.rsqrt(mean + 1e-06), (begun, LANES))
        if stage == 0:
            for index in range(pieces):
                first_weight_copy(index).wait()
            table_copies[1].wait()
        if stage == SPLIT - 1:
            for step in range(1, chunks):
                weight_copy(step).start()
            for copy in table_copies[2:]:
                copy.start()
        give_out(0, 0, part, jnp.dot(raw[part, :], held[0], preferred_element_type=jnp.float32))
        if stage == 0:
            arrive()
        send_out(0, 0, part)

    everything = pl.ds(0, rows)

    def chunk(step, carry):
        unit = step // HALVES
        number = step % HALVES
        weight_copy(step).wait()
        give_out(unit, number, everything, jnp.dot(raw[...], held[step], preferred_element_type=jnp.float32))
        send_out(unit, number, everything)
        return carry

    lax.fori_loop(1, chunks, chunk, 0)
    for unit in range(units):
        pltpu.make_async_copy(sent.at[unit, me], taken.at[unit, me], own_sem.at[unit]).start()
    out_copy.start()
    last_copy.start()

    for copy in table_copies[2:]:
        copy.wait()
    zeroth_here = me % places == 0

    @pl.when(zeroth_here)
    def _():
        table[...] = special[...]

    @pl.when(jnp.logical_not(zeroth_here))
    def _():
        table[...] = usual[...]

    def turned(slot):
        a = lax.dot_general(
            grid[slot], first[...], (((0,), (0,)), ((), ())), preferred_element_type=jnp.float32
        )
        re, im = a[:, :outer], a[:, outer:]
        c, s = turn_cos[...], turn_sin[...]
        return [(re * c + im * s).astype(jnp.bfloat16), (im * c - re * s).astype(jnp.bfloat16)]

    for unit in range(units):
        pltpu.make_async_copy(sent.at[unit, me], taken.at[unit, me], own_sem.at[unit]).wait()
        wait_for(taken.at[unit], recv_sem.at[unit], devices - 1)
        for part in range(outer // devices):
            piece_of = taken[unit, :, :, part * inner : (part + 1) * inner]
            grid[:, part * devices : (part + 1) * devices, :] = jnp.swapaxes(
                piece_of.astype(jnp.float32), 0, 1
            ).astype(jnp.bfloat16)
        for pair in range(pairs):
            b = jnp.concatenate(turned(pair) + turned(pair + pairs), axis=0)
            here_table = table if pair == 0 else usual
            o = jnp.dot(here_table[...], b, preferred_element_type=jnp.float32)
            done[pair] = o[:inner]
            done[pair + pairs] = o[inner:]
        for part in range(inner // devices):
            piece_of = done[:, part * devices : (part + 1) * devices, :]
            back[unit, :, :, part * outer : (part + 1) * outer] = jnp.swapaxes(piece_of, 0, 1).astype(jnp.bfloat16)
        for step in range(PLANES):
            send_plane(
                devices,
                step,
                back.at[unit],
                landed.at[unit],
                back_sem.at[unit],
                landed_sem.at[unit, step // HALVES],
                step // (PLANES - 1),
            )
        pltpu.make_async_copy(back.at[unit, me], landed.at[unit, me], own_back_sem.at[unit]).start()

    def put_in_order(unit, half):
        parts = landed[unit, pl.ds(half * members, members)].astype(jnp.float32)
        joined = parts.reshape(width, rows).astype(jnp.bfloat16)
        return lax.dot_general(
            joined, order[...], (((0,), (0,)), ((), ())), preferred_element_type=jnp.float32
        ).astype(jnp.bfloat16)

    tile = out_width // 8
    out_copy.wait()
    for unit in range(units):
        pltpu.make_async_copy(back.at[unit, me], landed.at[unit, me], own_back_sem.at[unit]).wait()
        for number in reversed(range(HALVES)):
            wait_for(landed.at[unit], landed_sem.at[unit, number], members - number)
            half = half_of(number)
            if unit == units - 1 and number == 0:
                last[...] = put_in_order(unit, half)
                continue
            ordered[...] = put_in_order(unit, half)
            begin = pl.multiple_of((unit * HALVES + half) * width, width)
            starting = unit == 0 and number == HALVES - 1

            def add_up(index, carry):
                across = pl.ds(pl.multiple_of(index * tile, tile), tile)
                product = jnp.dot(
                    ordered[...], held_out[pl.ds(begin, width), across], preferred_element_type=jnp.float32
                )
                total[:, across] = product if starting else total[:, across] + product
                return carry

            lax.fori_loop(0, out_width // tile, add_up, 0)

    last_copy.wait()
    for unit in range(units):
        wait_for(sent.at[unit], send_sem.at[unit], devices - 1)
        wait_for(back.at[unit], back_sem.at[unit], devices - 1)


def mixer(tokens, gain, weight, out_weight, forward, tables, order, units, devices):
    rows, depth = tokens.shape
    channels = weight.shape[1]
    slots = channels // devices // units
    outer = tables[0].shape[0]
    inner = tables[1].shape[0]
    width = channels // units // HALVES
    out_width = out_weight.shape[1]
    whole = pl.BlockSpec(memory_space=pltpu.VMEM)
    hbm = pl.BlockSpec(memory_space=pltpu.HBM)
    pieces = 4
    block = 16
    small = (gain, forward, *tables, order)
    return pl.pallas_call(
        functools.partial(mixer_kernel, devices),
        out_shape=(
            pltpu.VMEM((rows, out_width), jnp.float32),
            pltpu.VMEM((rows, width), jnp.bfloat16),
            pltpu.VMEM((width, out_width), jnp.bfloat16),
        ),
        in_specs=[hbm] * (3 + len(small)),
        out_specs=(whole, whole, whole),
        scratch_shapes=[pltpu.VMEM(table.shape, table.dtype) for table in small] + [
            pltpu.VMEM((rows, depth), jnp.bfloat16),
            pltpu.VMEM((units * HALVES, depth, width), jnp.bfloat16),
            pltpu.VMEM((channels, out_width), jnp.bfloat16),
            pltpu.VMEM((block, depth), jnp.bfloat16),
            pltpu.VMEM((rows, LANES), jnp.float32),
            pltpu.VMEM((units, devices, slots, rows), jnp.bfloat16),
            pltpu.VMEM((units, devices, slots, rows), jnp.bfloat16),
            pltpu.VMEM(tables[3].shape, jnp.bfloat16),
            pltpu.VMEM((slots, outer, inner), jnp.bfloat16),
            pltpu.VMEM((slots, inner, outer), jnp.float32),
            pltpu.VMEM((units, devices, slots, rows), jnp.bfloat16),
            pltpu.VMEM((units, devices, slots, rows), jnp.bfloat16),
            pltpu.VMEM((rows, width), jnp.bfloat16),
            pltpu.SemaphoreType.DMA((pieces,)),
            pltpu.SemaphoreType.DMA((pieces,)),
            pltpu.SemaphoreType.DMA((units * HALVES,)),
            pltpu.SemaphoreType.DMA,
            pltpu.SemaphoreType.DMA,
            pltpu.SemaphoreType.DMA((units,)),
            pltpu.SemaphoreType.DMA((units,)),
            pltpu.SemaphoreType.DMA((units,)),
            pltpu.SemaphoreType.DMA((units,)),
            pltpu.SemaphoreType.DMA((units,)),
            pltpu.SemaphoreType.DMA((units, HALVES)),
            pltpu.SemaphoreType.DMA((len(small),)),
        ],
        compiler_params=pltpu.CompilerParams(collective_id=0, has_side_effects=True, vmem_limit_bytes=46 << 20),
    )(*[pltpu.with_memory_space_constraint(array, pltpu.HBM) for array in (tokens, weight, out_weight, *small)])


def finish_kernel(total, last, last_weight, out, staged, sems):
    tiles = sems.shape[0]
    tile = staged.shape[1] // tiles

    def store(index):
        across = pl.ds(index * tile, tile)
        return pltpu.make_async_copy(staged.at[:, across], out.at[:, across], sems.at[index])

    for index in range(tiles):
        across = pl.ds(index * tile, tile)
        product = jnp.dot(last[...], last_weight[:, across], preferred_element_type=jnp.float32)
        staged[:, across] = (total[:, across] + product).astype(jnp.bfloat16)
        store(index).start()
    for index in range(tiles):
        store(index).wait()


def finish(total, last, last_weight):
    rows, out_width = total.shape
    tiles = 8
    whole = pl.BlockSpec(memory_space=pltpu.VMEM)
    return pl.pallas_call(
        finish_kernel,
        out_shape=pltpu.HBM((rows, out_width), jnp.bfloat16),
        in_specs=[whole] * 3,
        out_specs=pl.BlockSpec(memory_space=pltpu.HBM),
        scratch_shapes=[
            pltpu.VMEM((rows, out_width), jnp.bfloat16),
            pltpu.SemaphoreType.DMA((tiles,)),
        ],
        compiler_params=pltpu.CompilerParams(vmem_limit_bytes=20 << 20),
    )(total, last, last_weight)


def local(tokens, norm_gain, in_weight, out_weight):
    rows_here = tokens.shape[0]
    channels = in_weight.shape[1]
    devices = lax.axis_size(AXES)
    slots = channels // devices
    units = max(1, slots // 16)
    length = rows_here * devices
    inner = 1 << ((length.bit_length()) // 2)
    outer = length // inner

    forward, order = channel_tables(slots // units)
    several = np.eye(channels // units // HALVES // GROUP_WIDTH)
    forward = np.kron(several, forward.astype(np.float32)).astype(jnp.bfloat16)
    order = np.kron(several, order.astype(np.float32)).T.astype(jnp.bfloat16)
    tables = position_tables(outer, inner, devices)
    total, last, last_weight = mixer(
        tokens, norm_gain, in_weight, out_weight, forward, tables, order, units, devices
    )
    return finish(total, last, last_weight)


def solution(mesh):
    placed = (P(AXES, None), P(), P(), P())
    return jax.shard_map(
        local, mesh=mesh, in_specs=placed, out_specs=P(AXES, None), check_vma=False
    )
```

```python
import functools
import math

import jax
import jax.numpy as jnp
import numpy as np
from jax import lax
from jax.experimental import pallas as pl
from jax.experimental.pallas import tpu as pltpu
from jax.sharding import PartitionSpec as P

GROUP_WIDTH = 64
AXES = ("row", "col")


def channel_tables(slots):
    pairs = slots // 2
    half = GROUP_WIDTH // 2
    index = np.arange(GROUP_WIDTH)
    forward = np.zeros((GROUP_WIDTH, GROUP_WIDTH))
    order = np.zeros((GROUP_WIDTH, GROUP_WIDTH))
    for slot in range(GROUP_WIDTH):
        place, within = divmod(slot, slots)
        pair = place * pairs + within % pairs
        angles = 2.0 * math.pi / GROUP_WIDTH * (pair * index % GROUP_WIDTH)
        if within < pairs:
            forward[slot] = np.cos(angles)
            order[pair, slot] = 1.0
        elif pair == 0:
            forward[slot] = np.cos(math.pi * index)
            order[half, slot] = 1.0
        else:
            forward[slot] = np.sin(angles)
            order[GROUP_WIDTH - pair, slot] = 1.0
    forward /= math.sqrt(GROUP_WIDTH)
    return forward.astype(jnp.bfloat16), order.astype(jnp.bfloat16)


def position_tables(outer, inner, devices):
    length = outer * inner
    k1 = np.arange(outer)
    n2 = np.arange(inner)
    n1_order = k1.reshape(devices, -1).T.reshape(-1)
    k2_order = n2.reshape(devices, -1).T.reshape(-1)
    one = 2.0 * math.pi / outer * (np.outer(n1_order, k1) % outer)
    first = np.concatenate([np.cos(one), -np.sin(one)], axis=1)
    turn = 2.0 * math.pi / length * np.outer(n2, k1)
    two = 2.0 * math.pi / inner * (np.outer(k2_order, n2) % inner)
    scale = 1.0 / math.sqrt(length)
    c, s, z = np.cos(two) * scale, np.sin(two) * scale, np.zeros((inner, inner))
    usual = np.block([[c, s, -s, c], [c, s, s, -c]])
    zeroth = np.block([[c, s, z, z], [z, z, c, s]])
    return (
        first.astype(jnp.bfloat16),
        np.cos(turn).astype(np.float32),
        np.sin(turn).astype(np.float32),
        usual.astype(jnp.bfloat16),
        zeroth.astype(jnp.bfloat16),
    )


PLANES = 4
HALVES = 2
LANES = 128
MESH = pl.DeviceIdType.MESH


def place_of(device, columns):
    return (device // columns, device % columns)


def turned_plane(plane, step):
    high = (plane // 2 + 1 - step // 2) % 2
    low = (plane % 2 + (step + 1) // 2) % 2
    return 2 * high + low


def here(devices):
    columns = lax.axis_size("col")
    me = lax.axis_index("row") * columns + lax.axis_index("col")
    per = devices // PLANES
    return me, columns, per, me // per, me % per


def greet(devices):
    me, columns, _, _, _ = here(devices)
    barrier = pltpu.get_barrier_semaphore()

    def signal(step, carry):
        other = (me + step) % devices
        pl.semaphore_signal(barrier, inc=1, device_id=place_of(other, columns), device_id_type=MESH)
        return carry

    lax.fori_loop(1, devices, signal, 0)
    return lambda: pl.semaphore_wait(barrier, devices - 1)


def send_plane(devices, step, from_ref, to_ref, send_sem, recv_sem, first, across=slice(None)):
    me, columns, per, plane, lane = here(devices)
    target_plane = turned_plane(plane, step)

    def send(hop, carry):
        target = target_plane * per + (lane + hop) % per
        pltpu.make_async_remote_copy(
            src_ref=from_ref.at[target, :, across],
            dst_ref=to_ref.at[me, :, across],
            send_sem=send_sem,
            recv_sem=recv_sem,
            device_id=place_of(target, columns),
            device_id_type=MESH,
        ).start()
        return carry

    lax.fori_loop(first, per, send, 0)


def wait_for(ref, sem, count):
    part = ref.at[pl.ds(0, count)]
    pltpu.make_async_copy(part, part, sem).wait()


def mixer_kernel(
    devices,
    tokens,
    weight,
    out_weight,
    gain_hbm,
    forward_hbm,
    first_hbm,
    turn_cos_hbm,
    turn_sin_hbm,
    usual_hbm,
    special_hbm,
    order_hbm,
    total,
    last,
    last_weight,
    gain,
    forward,
    first,
    turn_cos,
    turn_sin,
    usual,
    special,
    order,
    raw,
    held,
    held_out,
    wide,
    squares,
    sent,
    taken,
    table,
    grid,
    done,
    back,
    landed,
    ordered,
    token_sem,
    first_weight_sem,
    weight_sem,
    out_sem,
    last_sem,
    own_sem,
    send_sem,
    recv_sem,
    own_back_sem,
    back_sem,
    landed_sem,
    table_sem,
):
    me, columns, per, plane, lane = here(devices)
    pieces = token_sem.shape[0]
    rows, depth = raw.shape
    piece = rows // pieces
    first_piece = depth // pieces
    width = held.shape[2]
    units, _, slots, _ = sent.shape
    members = devices // HALVES
    near = plane // HALVES
    far = (near + 1) % HALVES
    pairs = slots // 2
    places = GROUP_WIDTH // slots
    outer = first.shape[0]
    inner = turn_cos.shape[0]
    chunks = units * HALVES

    def token_copy(index):
        part = pl.ds(index * piece, piece)
        return pltpu.make_async_copy(tokens.at[part], raw.at[part], token_sem.at[index])

    def half_of(number):
        return (near + 1 + number) % HALVES

    def weight_copy(step):
        begin = pl.multiple_of((step // HALVES * HALVES + half_of(step % HALVES)) * width, width)
        return pltpu.make_async_copy(weight.at[:, pl.ds(begin, width)], held.at[step], weight_sem.at[step])

    def first_weight_copy(index):
        part = pl.ds(index * first_piece, first_piece)
        begin = pl.multiple_of(half_of(0) * width, width)
        return pltpu.make_async_copy(
            weight.at[part, pl.ds(begin, width)], held.at[0, part], first_weight_sem.at[index]
        )

    out_width = out_weight.shape[1]
    far_begin = pl.multiple_of(((units - 1) * HALVES + far) * width, width)
    out_copy = pltpu.make_async_copy(out_weight, held_out, out_sem)
    last_copy = pltpu.make_async_copy(out_weight.at[pl.ds(far_begin, width)], last_weight, last_sem)

    distant = (gain_hbm, forward_hbm, first_hbm, turn_cos_hbm, turn_sin_hbm, usual_hbm, special_hbm, order_hbm)
    nearby = (gain, forward, first, turn_cos, turn_sin, usual, special, order)
    table_copies = [
        pltpu.make_async_copy(a, b, table_sem.at[index]) for index, (a, b) in enumerate(zip(distant, nearby))
    ]
    table_copies[0].start()
    token_copy(0).start()
    arrive = greet(devices)
    for index in range(pieces):
        first_weight_copy(index).start()
    table_copies[1].start()

    block = wide.shape[0]
    table_copies[0].wait()
    wide[...] = jnp.broadcast_to(gain[...].astype(jnp.float32).reshape(1, depth), wide.shape).astype(jnp.bfloat16)

    def give_out(unit, number, part, product):
        half = half_of(number)
        scaling = jnp.concatenate([squares[part, :]] * (width // LANES), axis=1)
        hidden = (product * scaling).astype(jnp.bfloat16)
        spectrum = lax.dot_general(
            forward[...], hidden, (((1,), (1,)), ((), ())), preferred_element_type=jnp.float32
        )
        sent[unit, pl.ds(half * members, members), :, part] = spectrum.reshape(
            members, slots, part.size
        ).astype(jnp.bfloat16)

    def send_out(unit, number, part):
        for inside in range(PLANES // HALVES):
            plane_step = number * (PLANES // HALVES) + inside
            send_plane(
                devices,
                plane_step,
                sent.at[unit],
                taken.at[unit],
                send_sem.at[unit],
                recv_sem.at[unit],
                plane_step // (PLANES - 1),
                part,
            )

    def gather_squares(number, carry):
        part = pl.ds(pl.multiple_of(number * block, block), block)
        parts = [jnp.zeros((block, LANES), jnp.float32) for _ in range(4)]
        for column in range(depth // LANES):
            across = pl.ds(column * LANES, LANES)
            values = raw[part, across]
            floats = values.astype(jnp.float32)
            parts[column % 4] = parts[column % 4] + floats * floats
            raw[part, across] = values * wide[:, across]
        squares[part, :] = (parts[0] + parts[1]) + (parts[2] + parts[3])
        return carry

    stages = [(index, index + 1) for index in range(pieces)]
    for stage, (begin, end) in enumerate(stages):
        begun = (end - begin) * piece
        part = pl.ds(begin * piece, begun)
        for index in range(begin, end):
            token_copy(index).wait()
            if index == 0:
                for later in range(1, pieces):
                    token_copy(later).start()
            lax.fori_loop(index * piece // block, (index + 1) * piece // block, gather_squares, 0, unroll=2)
        mean = jnp.sum(squares[part, :], axis=-1, keepdims=True) * (1.0 / depth)
        squares[part, :] = jnp.broadcast_to(lax.rsqrt(mean + 1e-06), (begun, LANES))
        if stage == 0:
            for index in range(pieces):
                first_weight_copy(index).wait()
            table_copies[1].wait()
        if stage == len(stages) - 1:
            for step in range(1, chunks):
                weight_copy(step).start()
            for copy in table_copies[2:]:
                copy.start()
        give_out(0, 0, part, jnp.dot(raw[part, :], held[0], preferred_element_type=jnp.float32))
        if stage == 0:
            arrive()
        send_out(0, 0, part)

    everything = pl.ds(0, rows)

    def chunk(step, carry):
        unit = step // HALVES
        number = step % HALVES
        weight_copy(step).wait()
        give_out(unit, number, everything, jnp.dot(raw[...], held[step], preferred_element_type=jnp.float32))
        send_out(unit, number, everything)
        return carry

    lax.fori_loop(1, chunks, chunk, 0)
    for unit in range(units):
        pltpu.make_async_copy(sent.at[unit, me], taken.at[unit, me], own_sem.at[unit]).start()
    out_copy.start()
    last_copy.start()

    for copy in table_copies[2:]:
        copy.wait()
    zeroth_here = me % places == 0

    @pl.when(zeroth_here)
    def _():
        table[...] = special[...]

    @pl.when(jnp.logical_not(zeroth_here))
    def _():
        table[...] = usual[...]

    def turned(slot):
        a = lax.dot_general(
            grid[slot], first[...], (((0,), (0,)), ((), ())), preferred_element_type=jnp.float32
        )
        re, im = a[:, :outer], a[:, outer:]
        c, s = turn_cos[...], turn_sin[...]
        return [(re * c + im * s).astype(jnp.bfloat16), (im * c - re * s).astype(jnp.bfloat16)]

    for unit in range(units):
        pltpu.make_async_copy(sent.at[unit, me], taken.at[unit, me], own_sem.at[unit]).wait()
        wait_for(taken.at[unit], recv_sem.at[unit], devices - 1)
        for part in range(outer // devices):
            piece_of = taken[unit, :, :, part * inner : (part + 1) * inner]
            grid[:, part * devices : (part + 1) * devices, :] = jnp.swapaxes(
                piece_of.astype(jnp.float32), 0, 1
            ).astype(jnp.bfloat16)
        for pair in range(pairs):
            b = jnp.concatenate(turned(pair) + turned(pair + pairs), axis=0)
            here_table = table if pair == 0 else usual
            o = jnp.dot(here_table[...], b, preferred_element_type=jnp.float32)
            done[pair] = o[:inner]
            done[pair + pairs] = o[inner:]
        for part in range(inner // devices):
            piece_of = done[:, part * devices : (part + 1) * devices, :]
            back[unit, :, :, part * outer : (part + 1) * outer] = jnp.swapaxes(piece_of, 0, 1).astype(jnp.bfloat16)
        for step in range(PLANES):
            send_plane(
                devices,
                step,
                back.at[unit],
                landed.at[unit],
                back_sem.at[unit],
                landed_sem.at[unit, step // HALVES],
                step // (PLANES - 1),
            )
        pltpu.make_async_copy(back.at[unit, me], landed.at[unit, me], own_back_sem.at[unit]).start()

    def put_in_order(unit, half):
        parts = landed[unit, pl.ds(half * members, members)].astype(jnp.float32)
        joined = parts.reshape(width, rows).astype(jnp.bfloat16)
        return lax.dot_general(
            joined, order[...], (((0,), (0,)), ((), ())), preferred_element_type=jnp.float32
        ).astype(jnp.bfloat16)

    tile = out_width // 8
    out_copy.wait()
    for unit in range(units):
        pltpu.make_async_copy(back.at[unit, me], landed.at[unit, me], own_back_sem.at[unit]).wait()
        for number in reversed(range(HALVES)):
            wait_for(landed.at[unit], landed_sem.at[unit, number], members - number)
            half = half_of(number)
            if unit == units - 1 and number == 0:
                last[...] = put_in_order(unit, half)
                continue
            ordered[...] = put_in_order(unit, half)
            begin = pl.multiple_of((unit * HALVES + half) * width, width)
            starting = unit == 0 and number == HALVES - 1

            def add_up(index, carry):
                across = pl.ds(pl.multiple_of(index * tile, tile), tile)
                product = jnp.dot(
                    ordered[...], held_out[pl.ds(begin, width), across], preferred_element_type=jnp.float32
                )
                total[:, across] = product if starting else total[:, across] + product
                return carry

            lax.fori_loop(0, out_width // tile, add_up, 0)

    last_copy.wait()
    for unit in range(units):
        wait_for(sent.at[unit], send_sem.at[unit], devices - 1)
        wait_for(back.at[unit], back_sem.at[unit], devices - 1)


def mixer(tokens, gain, weight, out_weight, forward, tables, order, units, devices):
    rows, depth = tokens.shape
    channels = weight.shape[1]
    slots = channels // devices // units
    outer = tables[0].shape[0]
    inner = tables[1].shape[0]
    width = channels // units // HALVES
    out_width = out_weight.shape[1]
    whole = pl.BlockSpec(memory_space=pltpu.VMEM)
    hbm = pl.BlockSpec(memory_space=pltpu.HBM)
    pieces = 4
    block = 16
    small = (gain, forward, *tables, order)
    return pl.pallas_call(
        functools.partial(mixer_kernel, devices),
        out_shape=(
            pltpu.VMEM((rows, out_width), jnp.float32),
            pltpu.VMEM((rows, width), jnp.bfloat16),
            pltpu.VMEM((width, out_width), jnp.bfloat16),
        ),
        in_specs=[hbm] * (3 + len(small)),
        out_specs=(whole, whole, whole),
        scratch_shapes=[pltpu.VMEM(table.shape, table.dtype) for table in small] + [
            pltpu.VMEM((rows, depth), jnp.bfloat16),
            pltpu.VMEM((units * HALVES, depth, width), jnp.bfloat16),
            pltpu.VMEM((channels, out_width), jnp.bfloat16),
            pltpu.VMEM((block, depth), jnp.bfloat16),
            pltpu.VMEM((rows, LANES), jnp.float32),
            pltpu.VMEM((units, devices, slots, rows), jnp.bfloat16),
            pltpu.VMEM((units, devices, slots, rows), jnp.bfloat16),
            pltpu.VMEM(tables[3].shape, jnp.bfloat16),
            pltpu.VMEM((slots, outer, inner), jnp.bfloat16),
            pltpu.VMEM((slots, inner, outer), jnp.float32),
            pltpu.VMEM((units, devices, slots, rows), jnp.bfloat16),
            pltpu.VMEM((units, devices, slots, rows), jnp.bfloat16),
            pltpu.VMEM((rows, width), jnp.bfloat16),
            pltpu.SemaphoreType.DMA((pieces,)),
            pltpu.SemaphoreType.DMA((pieces,)),
            pltpu.SemaphoreType.DMA((units * HALVES,)),
            pltpu.SemaphoreType.DMA,
            pltpu.SemaphoreType.DMA,
            pltpu.SemaphoreType.DMA((units,)),
            pltpu.SemaphoreType.DMA((units,)),
            pltpu.SemaphoreType.DMA((units,)),
            pltpu.SemaphoreType.DMA((units,)),
            pltpu.SemaphoreType.DMA((units,)),
            pltpu.SemaphoreType.DMA((units, HALVES)),
            pltpu.SemaphoreType.DMA((len(small),)),
        ],
        compiler_params=pltpu.CompilerParams(collective_id=0, has_side_effects=True, vmem_limit_bytes=46 << 20),
    )(*[pltpu.with_memory_space_constraint(array, pltpu.HBM) for array in (tokens, weight, out_weight, *small)])


def finish_kernel(total, last, last_weight, out, staged, sems):
    tiles = sems.shape[0]
    tile = staged.shape[1] // tiles

    def store(index):
        across = pl.ds(index * tile, tile)
        return pltpu.make_async_copy(staged.at[:, across], out.at[:, across], sems.at[index])

    for index in range(tiles):
        across = pl.ds(index * tile, tile)
        product = jnp.dot(last[...], last_weight[:, across], preferred_element_type=jnp.float32)
        staged[:, across] = (total[:, across] + product).astype(jnp.bfloat16)
        store(index).start()
    for index in range(tiles):
        store(index).wait()


def finish(total, last, last_weight):
    rows, out_width = total.shape
    tiles = 8
    whole = pl.BlockSpec(memory_space=pltpu.VMEM)
    return pl.pallas_call(
        finish_kernel,
        out_shape=pltpu.HBM((rows, out_width), jnp.bfloat16),
        in_specs=[whole] * 3,
        out_specs=pl.BlockSpec(memory_space=pltpu.HBM),
        scratch_shapes=[
            pltpu.VMEM((rows, out_width), jnp.bfloat16),
            pltpu.SemaphoreType.DMA((tiles,)),
        ],
        compiler_params=pltpu.CompilerParams(vmem_limit_bytes=20 << 20),
    )(total, last, last_weight)


def local(tokens, norm_gain, in_weight, out_weight):
    rows_here = tokens.shape[0]
    channels = in_weight.shape[1]
    devices = lax.axis_size(AXES)
    slots = channels // devices
    units = max(1, slots // 16)
    length = rows_here * devices
    inner = 1 << ((length.bit_length()) // 2)
    outer = length // inner

    forward, order = channel_tables(slots // units)
    several = np.eye(channels // units // HALVES // GROUP_WIDTH)
    forward = np.kron(several, forward.astype(np.float32)).astype(jnp.bfloat16)
    order = np.kron(several, order.astype(np.float32)).T.astype(jnp.bfloat16)
    tables = position_tables(outer, inner, devices)
    total, last, last_weight = mixer(
        tokens, norm_gain, in_weight, out_weight, forward, tables, order, units, devices
    )
    return finish(total, last, last_weight)


def solution(mesh):
    placed = (P(AXES, None), P(), P(), P())
    return jax.shard_map(
        local, mesh=mesh, in_specs=placed, out_specs=P(AXES, None), check_vma=False
    )
```

```python
import functools
import itertools
import math

import jax
import jax.numpy as jnp
import numpy as np
from jax import lax
from jax.experimental import pallas as pl
from jax.experimental.pallas import tpu as pltpu
from jax.sharding import PartitionSpec as P

GROUP_WIDTH = 64
AXES = ("row", "col")


def channel_tables(slots):
    pairs = slots // 2
    half = GROUP_WIDTH // 2
    index = np.arange(GROUP_WIDTH)
    forward = np.zeros((GROUP_WIDTH, GROUP_WIDTH))
    order = np.zeros((GROUP_WIDTH, GROUP_WIDTH))
    for slot in range(GROUP_WIDTH):
        place, within = divmod(slot, slots)
        pair = place * pairs + within % pairs
        angles = 2.0 * math.pi / GROUP_WIDTH * (pair * index % GROUP_WIDTH)
        if within < pairs:
            forward[slot] = np.cos(angles)
            order[pair, slot] = 1.0
        elif pair == 0:
            forward[slot] = np.cos(math.pi * index)
            order[half, slot] = 1.0
        else:
            forward[slot] = np.sin(angles)
            order[GROUP_WIDTH - pair, slot] = 1.0
    forward /= math.sqrt(GROUP_WIDTH)
    return forward.astype(jnp.bfloat16), order.astype(jnp.bfloat16)


def position_tables(outer, inner, devices):
    length = outer * inner
    k1 = np.arange(outer)
    n2 = np.arange(inner)
    n1_order = k1.reshape(devices, -1).T.reshape(-1)
    k2_order = n2.reshape(devices, -1).T.reshape(-1)
    one = 2.0 * math.pi / outer * (np.outer(n1_order, k1) % outer)
    first = np.concatenate([np.cos(one), -np.sin(one)], axis=1)
    turn = 2.0 * math.pi / length * np.outer(n2, k1)
    two = 2.0 * math.pi / inner * (np.outer(k2_order, n2) % inner)
    scale = 1.0 / math.sqrt(length)
    c, s, z = np.cos(two) * scale, np.sin(two) * scale, np.zeros((inner, inner))
    usual = np.block([[c, s, -s, c], [c, s, s, -c]])
    zeroth = np.block([[c, s, z, z], [z, z, c, s]])
    return (
        first.astype(jnp.bfloat16),
        np.cos(turn).astype(np.float32),
        np.sin(turn).astype(np.float32),
        usual.astype(jnp.bfloat16),
        zeroth.astype(jnp.bfloat16),
    )


PLANES = 4
HALVES = 2
CUTS = 2
LANES = 128
MESH = pl.DeviceIdType.MESH


def place_of(device, columns):
    return (device // columns, device % columns)


def turned_plane(plane, step):
    high = (plane // 2 + 1 - step // 2) % 2
    low = (plane % 2 + (step + 1) // 2) % 2
    return 2 * high + low


def here(devices):
    columns = lax.axis_size("col")
    me = lax.axis_index("row") * columns + lax.axis_index("col")
    per = devices // PLANES
    return me, columns, per, me // per, me % per


def greet(devices):
    me, columns, _, _, _ = here(devices)
    barrier = pltpu.get_barrier_semaphore()

    def signal(step, carry):
        other = (me + step) % devices
        pl.semaphore_signal(barrier, inc=1, device_id=place_of(other, columns), device_id_type=MESH)
        return carry

    lax.fori_loop(1, devices, signal, 0)
    return lambda: pl.semaphore_wait(barrier, devices - 1)


def send_plane(devices, step, from_ref, to_ref, send_sem, recv_sem, first, across=slice(None)):
    me, columns, per, plane, lane = here(devices)
    target_plane = turned_plane(plane, step)

    def send(hop, carry):
        target = target_plane * per + (lane + hop) % per
        pltpu.make_async_remote_copy(
            src_ref=from_ref.at[target, :, across],
            dst_ref=to_ref.at[me, :, across],
            send_sem=send_sem,
            recv_sem=recv_sem,
            device_id=place_of(target, columns),
            device_id_type=MESH,
        ).start()
        return carry

    lax.fori_loop(first, per, send, 0)


def send_far(devices, place, lanes, from_ref, to_ref, send_sem, recv_sem, across=slice(None)):
    me, columns, per, plane, lane = here(devices)
    low = plane // 2
    target_plane = (1 - low) * (2 + place) + low * ((plane % 2 + place) % 2)
    quarter = per // 4

    def send(hop, carry):
        spot = (lane + hop) % (per // 2)
        target_lane = (1 - lanes) * (spot + spot // quarter * 2 * quarter) + lanes * (quarter + spot)
        target = target_plane * per + target_lane
        pltpu.make_async_remote_copy(
            src_ref=from_ref.at[target, :, across],
            dst_ref=to_ref.at[me, :, across],
            send_sem=send_sem,
            recv_sem=recv_sem,
            device_id=place_of(target, columns),
            device_id_type=MESH,
        ).start()
        return carry

    lax.fori_loop(0, per // 2, send, 0)


def wait_for(ref, sem, count):
    part = ref.at[pl.ds(0, count)]
    pltpu.make_async_copy(part, part, sem).wait()


def put_in_order(joined, order):
    return lax.dot_general(
        joined, order[...], (((0,), (0,)), ((), ())), preferred_element_type=jnp.float32
    ).astype(jnp.bfloat16)


def mixer_kernel(
    devices,
    tokens,
    weight,
    out_weight,
    gain_hbm,
    forward_hbm,
    first_hbm,
    turn_cos_hbm,
    turn_sin_hbm,
    usual_hbm,
    special_hbm,
    order_hbm,
    total,
    last,
    last_weight,
    early,
    order,
    gain,
    forward,
    first,
    turn_cos,
    turn_sin,
    usual,
    special,
    raw,
    held,
    held_out,
    wide,
    squares,
    sent,
    taken,
    table,
    grid,
    done,
    back,
    landed,
    ordered,
    token_sem,
    first_weight_sem,
    weight_sem,
    out_sem,
    last_sem,
    own_sem,
    send_sem,
    recv_sem,
    own_back_sem,
    back_sem,
    landed_sem,
    table_sem,
):
    me, columns, per, plane, lane = here(devices)
    pieces = token_sem.shape[0]
    rows, depth = raw.shape
    piece = rows // pieces
    first_piece = depth // pieces
    width = held.shape[2]
    units, _, slots, _ = sent.shape
    members = devices // HALVES
    near = plane // HALVES
    far = (near + 1) % HALVES
    pairs = slots // 2
    places = GROUP_WIDTH // slots
    outer = first.shape[0]
    inner = turn_cos.shape[0]
    chunks = units * HALVES
    cut_rows = rows // CUTS

    def token_copy(index):
        part = pl.ds(index * piece, piece)
        return pltpu.make_async_copy(tokens.at[part], raw.at[part], token_sem.at[index])

    def half_of(number):
        return (near + 1 + number) % HALVES

    def weight_copy(step):
        begin = pl.multiple_of((step // HALVES * HALVES + half_of(step % HALVES)) * width, width)
        return pltpu.make_async_copy(weight.at[:, pl.ds(begin, width)], held.at[step], weight_sem.at[step])

    def first_weight_copy(index):
        part = pl.ds(index * first_piece, first_piece)
        begin = pl.multiple_of(half_of(0) * width, width)
        return pltpu.make_async_copy(
            weight.at[part, pl.ds(begin, width)], held.at[0, part], first_weight_sem.at[index]
        )

    out_width = out_weight.shape[1]
    far_begin = pl.multiple_of(((units - 1) * HALVES + far) * width, width)
    out_copy = pltpu.make_async_copy(out_weight, held_out, out_sem)
    last_copy = pltpu.make_async_copy(out_weight.at[pl.ds(far_begin, width)], last_weight, last_sem)

    distant = (gain_hbm, forward_hbm, first_hbm, turn_cos_hbm, turn_sin_hbm, usual_hbm, special_hbm, order_hbm)
    nearby = (gain, forward, first, turn_cos, turn_sin, usual, special, order)
    table_copies = [
        pltpu.make_async_copy(a, b, table_sem.at[index]) for index, (a, b) in enumerate(zip(distant, nearby))
    ]
    table_copies[0].start()
    token_copy(0).start()
    arrive = greet(devices)
    for index in range(pieces):
        first_weight_copy(index).start()
    table_copies[1].start()

    block = wide.shape[0]
    table_copies[0].wait()
    wide[...] = jnp.broadcast_to(gain[...].astype(jnp.float32).reshape(1, depth), wide.shape).astype(jnp.bfloat16)

    def give_out(unit, number, part, product):
        half = half_of(number)
        scaling = jnp.concatenate([squares[part, :]] * (width // LANES), axis=1)
        hidden = (product * scaling).astype(jnp.bfloat16)
        spectrum = lax.dot_general(
            forward[...], hidden, (((1,), (1,)), ((), ())), preferred_element_type=jnp.float32
        )
        sent[unit, pl.ds(half * members, members), :, part] = spectrum.reshape(
            members, slots, part.size
        ).astype(jnp.bfloat16)

    def send_out(unit, number, part):
        for inside in range(PLANES // HALVES):
            plane_step = number * (PLANES // HALVES) + inside
            send_plane(
                devices,
                plane_step,
                sent.at[unit],
                taken.at[unit],
                send_sem.at[unit],
                recv_sem.at[unit],
                plane_step // (PLANES - 1),
                part,
            )

    def gather_squares(number, carry):
        part = pl.ds(pl.multiple_of(number * block, block), block)
        parts = [jnp.zeros((block, LANES), jnp.float32) for _ in range(4)]
        for column in range(depth // LANES):
            across = pl.ds(column * LANES, LANES)
            values = raw[part, across]
            floats = values.astype(jnp.float32)
            parts[column % 4] = parts[column % 4] + floats * floats
            raw[part, across] = values * wide[:, across]
        squares[part, :] = (parts[0] + parts[1]) + (parts[2] + parts[3])
        return carry

    stages = [(index, index + 1) for index in range(pieces)]
    for stage, (begin, end) in enumerate(stages):
        begun = (end - begin) * piece
        part = pl.ds(begin * piece, begun)
        for index in range(begin, end):
            token_copy(index).wait()
            if index == 0:
                for later in range(1, pieces):
                    token_copy(later).start()
            lax.fori_loop(index * piece // block, (index + 1) * piece // block, gather_squares, 0, unroll=2)
        mean = jnp.sum(squares[part, :], axis=-1, keepdims=True) * (1.0 / depth)
        squares[part, :] = jnp.broadcast_to(lax.rsqrt(mean + 1e-06), (begun, LANES))
        if stage == 0:
            for index in range(pieces):
                first_weight_copy(index).wait()
            table_copies[1].wait()
        if stage == len(stages) - 1:
            for step in range(1, chunks):
                weight_copy(step).start()
            for copy in table_copies[2:]:
                copy.start()
        give_out(0, 0, part, jnp.dot(raw[part, :], held[0], preferred_element_type=jnp.float32))
        if stage == 0:
            arrive()
        send_out(0, 0, part)

    everything = pl.ds(0, rows)

    def chunk(step, carry):
        unit = step // HALVES
        number = step % HALVES
        weight_copy(step).wait()
        give_out(unit, number, everything, jnp.dot(raw[...], held[step], preferred_element_type=jnp.float32))
        send_out(unit, number, everything)
        return carry

    lax.fori_loop(1, chunks, chunk, 0)
    for unit in range(units):
        pltpu.make_async_copy(sent.at[unit, me], taken.at[unit, me], own_sem.at[unit]).start()
    out_copy.start()
    last_copy.start()

    for copy in table_copies[2:]:
        copy.wait()
    zeroth_here = me % places == 0

    @pl.when(zeroth_here)
    def _():
        table[...] = special[...]

    @pl.when(jnp.logical_not(zeroth_here))
    def _():
        table[...] = usual[...]

    def turned(slot):
        a = lax.dot_general(
            grid[slot], first[...], (((0,), (0,)), ((), ())), preferred_element_type=jnp.float32
        )
        re, im = a[:, :outer], a[:, outer:]
        c, s = turn_cos[...], turn_sin[...]
        return [(re * c + im * s).astype(jnp.bfloat16), (im * c - re * s).astype(jnp.bfloat16)]

    for unit in range(units):
        pltpu.make_async_copy(sent.at[unit, me], taken.at[unit, me], own_sem.at[unit]).wait()
        wait_for(taken.at[unit], recv_sem.at[unit], devices - 1)
        for part in range(outer // devices):
            piece_of = taken[unit, :, :, part * inner : (part + 1) * inner]
            grid[:, part * devices : (part + 1) * devices, :] = jnp.swapaxes(
                piece_of.astype(jnp.float32), 0, 1
            ).astype(jnp.bfloat16)
        for pair in range(pairs):
            b = jnp.concatenate(turned(pair) + turned(pair + pairs), axis=0)
            here_table = table if pair == 0 else usual
            o = jnp.dot(here_table[...], b, preferred_element_type=jnp.float32)
            done[pair] = o[:inner]
            done[pair + pairs] = o[inner:]
        for part in range(inner // devices):
            piece_of = done[:, part * devices : (part + 1) * devices, :]
            back[unit, :, :, part * outer : (part + 1) * outer] = jnp.swapaxes(piece_of, 0, 1).astype(jnp.bfloat16)
        last_unit = unit == units - 1
        for place, cut, lanes in itertools.product(range(2), range(CUTS if last_unit else 1), range(2)):
            send_far(
                devices,
                place,
                lanes,
                back.at[unit],
                landed.at[unit],
                back_sem.at[unit],
                landed_sem.at[unit, cut],
                pl.ds(cut * cut_rows, cut_rows) if last_unit else slice(None),
            )
        for step in range(HALVES, PLANES):
            send_plane(
                devices,
                step,
                back.at[unit],
                landed.at[unit],
                back_sem.at[unit],
                landed_sem.at[unit, CUTS],
                step // (PLANES - 1),
            )
        pltpu.make_async_copy(back.at[unit, me], landed.at[unit, me], own_back_sem.at[unit]).start()

    def joined(unit, half, across):
        parts = landed[unit, pl.ds(half * members, members), :, across].astype(jnp.float32)
        return parts.reshape(width, parts.shape[2]).astype(jnp.bfloat16)

    tile = out_width // 4
    tiles = out_width // tile
    out_copy.wait()
    for unit in range(units):
        pltpu.make_async_copy(back.at[unit, me], landed.at[unit, me], own_back_sem.at[unit]).wait()
        for number in reversed(range(HALVES)):
            half = half_of(number)
            begin = pl.multiple_of((unit * HALVES + half) * width, width)
            closing = unit == units - 1 and number == 0
            starting = unit == 0 and number == HALVES - 1
            part = pl.ds(0, cut_rows) if closing else pl.ds(0, rows)
            if closing:
                wait_for(landed.at[unit, :, :, part], landed_sem.at[unit, 0], members)
            else:
                wait_for(landed.at[unit], landed_sem.at[unit, CUTS * number], members - number)
            ordered[part, :] = put_in_order(joined(unit, half, part), order)

            def add_up(index, carry):
                across = pl.ds(pl.multiple_of(index * tile, tile), tile)
                product = jnp.dot(
                    ordered[part, :], held_out[pl.ds(begin, width), across], preferred_element_type=jnp.float32
                )
                if closing:
                    early[:, across] = (total[part, across] + product).astype(jnp.bfloat16)
                else:
                    total[:, across] = product if starting else total[:, across] + product
                return carry

            lax.fori_loop(0, tiles, add_up, 0)

    last_copy.wait()
    rest = pl.ds(cut_rows, cut_rows)
    wait_for(landed.at[units - 1, :, :, rest], landed_sem.at[units - 1, 1], members)
    last[...] = joined(units - 1, half_of(0), rest)
    for unit in range(units):
        wait_for(sent.at[unit], send_sem.at[unit], devices - 1)
        wait_for(back.at[unit], back_sem.at[unit], devices - 1)


def mixer(tokens, gain, weight, out_weight, forward, tables, order, units, devices):
    rows, depth = tokens.shape
    channels = weight.shape[1]
    slots = channels // devices // units
    outer = tables[0].shape[0]
    inner = tables[1].shape[0]
    width = channels // units // HALVES
    out_width = out_weight.shape[1]
    whole = pl.BlockSpec(memory_space=pltpu.VMEM)
    hbm = pl.BlockSpec(memory_space=pltpu.HBM)
    pieces = 4
    block = 16
    small = (gain, forward, *tables, order)
    return pl.pallas_call(
        functools.partial(mixer_kernel, devices),
        out_shape=(
            pltpu.VMEM((rows, out_width), jnp.float32),
            pltpu.VMEM((width, rows // CUTS), jnp.bfloat16),
            pltpu.VMEM((width, out_width), jnp.bfloat16),
            pltpu.VMEM((rows // CUTS, out_width), jnp.bfloat16),
            pltpu.VMEM(order.shape, order.dtype),
        ),
        in_specs=[hbm] * (3 + len(small)),
        out_specs=(whole,) * 5,
        scratch_shapes=[pltpu.VMEM(table.shape, table.dtype) for table in small[:-1]] + [
            pltpu.VMEM((rows, depth), jnp.bfloat16),
            pltpu.VMEM((units * HALVES, depth, width), jnp.bfloat16),
            pltpu.VMEM((channels, out_width), jnp.bfloat16),
            pltpu.VMEM((block, depth), jnp.bfloat16),
            pltpu.VMEM((rows, LANES), jnp.float32),
            pltpu.VMEM((units, devices, slots, rows), jnp.bfloat16),
            pltpu.VMEM((units, devices, slots, rows), jnp.bfloat16),
            pltpu.VMEM(tables[3].shape, jnp.bfloat16),
            pltpu.VMEM((slots, outer, inner), jnp.bfloat16),
            pltpu.VMEM((slots, inner, outer), jnp.float32),
            pltpu.VMEM((units, devices, slots, rows), jnp.bfloat16),
            pltpu.VMEM((units, devices, slots, rows), jnp.bfloat16),
            pltpu.VMEM((rows, width), jnp.bfloat16),
            pltpu.SemaphoreType.DMA((pieces,)),
            pltpu.SemaphoreType.DMA((pieces,)),
            pltpu.SemaphoreType.DMA((units * HALVES,)),
            pltpu.SemaphoreType.DMA,
            pltpu.SemaphoreType.DMA,
            pltpu.SemaphoreType.DMA((units,)),
            pltpu.SemaphoreType.DMA((units,)),
            pltpu.SemaphoreType.DMA((units,)),
            pltpu.SemaphoreType.DMA((units,)),
            pltpu.SemaphoreType.DMA((units,)),
            pltpu.SemaphoreType.DMA((units, CUTS + 1)),
            pltpu.SemaphoreType.DMA((len(small),)),
        ],
        compiler_params=pltpu.CompilerParams(collective_id=0, has_side_effects=True, vmem_limit_bytes=46 << 20),
    )(*[pltpu.with_memory_space_constraint(array, pltpu.HBM) for array in (tokens, weight, out_weight, *small)])


def finish_kernel(total, last, last_weight, early, order, out, staged, ordered, sems, early_sem):
    tiles = sems.shape[0]
    begin, out_width = staged.shape
    tile = out_width // tiles
    early_copy = pltpu.make_async_copy(early, out.at[pl.ds(0, begin)], early_sem)
    early_copy.start()
    ordered[...] = put_in_order(last[...], order)

    def store(index):
        across = pl.ds(index * tile, tile)
        return pltpu.make_async_copy(staged.at[:, across], out.at[pl.ds(begin, begin), across], sems.at[index])

    for index in range(tiles):
        across = pl.ds(index * tile, tile)
        product = jnp.dot(ordered[...], last_weight[:, across], preferred_element_type=jnp.float32)
        staged[:, across] = (total[pl.ds(begin, begin), across] + product).astype(jnp.bfloat16)
        store(index).start()
    early_copy.wait()
    for index in range(tiles):
        store(index).wait()


def finish(total, last, last_weight, early, order):
    rows, out_width = total.shape
    width = last_weight.shape[0]
    tiles = 4
    whole = pl.BlockSpec(memory_space=pltpu.VMEM)
    return pl.pallas_call(
        finish_kernel,
        out_shape=pltpu.HBM((rows, out_width), jnp.bfloat16),
        in_specs=[whole] * 5,
        out_specs=pl.BlockSpec(memory_space=pltpu.HBM),
        scratch_shapes=[
            pltpu.VMEM((rows // CUTS, out_width), jnp.bfloat16),
            pltpu.VMEM((rows // CUTS, width), jnp.bfloat16),
            pltpu.SemaphoreType.DMA((tiles,)),
            pltpu.SemaphoreType.DMA,
        ],
        compiler_params=pltpu.CompilerParams(vmem_limit_bytes=20 << 20),
    )(total, last, last_weight, early, order)


def local(tokens, norm_gain, in_weight, out_weight):
    rows_here = tokens.shape[0]
    channels = in_weight.shape[1]
    devices = lax.axis_size(AXES)
    slots = channels // devices
    units = max(1, slots // 16)
    length = rows_here * devices
    inner = 1 << ((length.bit_length()) // 2)
    outer = length // inner

    forward, order = channel_tables(slots // units)
    several = np.eye(channels // units // HALVES // GROUP_WIDTH)
    forward = np.kron(several, forward.astype(np.float32)).astype(jnp.bfloat16)
    order = np.kron(several, order.astype(np.float32)).T.astype(jnp.bfloat16)
    tables = position_tables(outer, inner, devices)
    parts = mixer(tokens, norm_gain, in_weight, out_weight, forward, tables, order, units, devices)
    return finish(*parts)


def solution(mesh):
    placed = (P(AXES, None), P(), P(), P())
    return jax.shard_map(
        local, mesh=mesh, in_specs=placed, out_specs=P(AXES, None), check_vma=False
    )
```

```python
import functools
import itertools
import math

import jax
import jax.numpy as jnp
import numpy as np
from jax import lax
from jax.experimental import pallas as pl
from jax.experimental.pallas import tpu as pltpu
from jax.sharding import PartitionSpec as P

GROUP_WIDTH = 64
AXES = ("row", "col")


def channel_tables(slots):
    pairs = slots // 2
    half = GROUP_WIDTH // 2
    index = np.arange(GROUP_WIDTH)
    forward = np.zeros((GROUP_WIDTH, GROUP_WIDTH))
    order = np.zeros((GROUP_WIDTH, GROUP_WIDTH))
    for slot in range(GROUP_WIDTH):
        place, within = divmod(slot, slots)
        pair = place * pairs + within % pairs
        angles = 2.0 * math.pi / GROUP_WIDTH * (pair * index % GROUP_WIDTH)
        if within < pairs:
            forward[slot] = np.cos(angles)
            order[pair, slot] = 1.0
        elif pair == 0:
            forward[slot] = np.cos(math.pi * index)
            order[half, slot] = 1.0
        else:
            forward[slot] = np.sin(angles)
            order[GROUP_WIDTH - pair, slot] = 1.0
    forward /= math.sqrt(GROUP_WIDTH)
    return forward.astype(jnp.bfloat16), order.astype(jnp.bfloat16)


def high_low(table, axis):
    high = table.astype(jnp.bfloat16)
    low = (table - high.astype(np.float64)).astype(jnp.bfloat16)
    return np.concatenate([high, low], axis=axis)


def position_tables(outer, inner, devices):
    length = outer * inner
    k1 = np.arange(outer)
    n2 = np.arange(inner)
    n1_order = k1.reshape(devices, -1).T.reshape(-1)
    k2_order = n2.reshape(devices, -1).T.reshape(-1)
    one = 2.0 * math.pi / outer * (np.outer(n1_order, k1) % outer)
    first = np.concatenate([np.cos(one), -np.sin(one)], axis=1)
    turn = 2.0 * math.pi / length * np.outer(n2, k1)
    two = 2.0 * math.pi / inner * (np.outer(k2_order, n2) % inner)
    scale = 1.0 / math.sqrt(length)
    c, s, z = np.cos(two) * scale, np.sin(two) * scale, np.zeros((inner, inner))
    usual = np.block([[c, s, -s, c], [c, s, s, -c]])
    zeroth = np.block([[c, s, z, z], [z, z, c, s]])
    return (
        high_low(first, 1),
        np.cos(turn).astype(np.float32),
        np.sin(turn).astype(np.float32),
        high_low(usual, 0),
        high_low(zeroth, 0),
    )


PLANES = 4
HALVES = 2
CUTS = 2
LANES = 128
MESH = pl.DeviceIdType.MESH


def place_of(device, columns):
    return (device // columns, device % columns)


def turned_plane(plane, step):
    high = (plane // 2 + 1 - step // 2) % 2
    low = (plane % 2 + (step + 1) // 2) % 2
    return 2 * high + low


def here(devices):
    columns = lax.axis_size("col")
    me = lax.axis_index("row") * columns + lax.axis_index("col")
    per = devices // PLANES
    return me, columns, per, me // per, me % per


def greet(devices):
    me, columns, _, _, _ = here(devices)
    barrier = pltpu.get_barrier_semaphore()

    def signal(step, carry):
        other = (me + step) % devices
        pl.semaphore_signal(barrier, inc=1, device_id=place_of(other, columns), device_id_type=MESH)
        return carry

    lax.fori_loop(1, devices, signal, 0)
    return lambda: pl.semaphore_wait(barrier, devices - 1)


def send_plane(devices, step, from_ref, to_ref, send_sem, recv_sem, first, across=slice(None)):
    me, columns, per, plane, lane = here(devices)
    target_plane = turned_plane(plane, step)

    def send(hop, carry):
        target = target_plane * per + (lane + hop) % per
        pltpu.make_async_remote_copy(
            src_ref=from_ref.at[target, :, across],
            dst_ref=to_ref.at[me, :, across],
            send_sem=send_sem,
            recv_sem=recv_sem,
            device_id=place_of(target, columns),
            device_id_type=MESH,
        ).start()
        return carry

    lax.fori_loop(first, per, send, 0)


def send_far(devices, place, lanes, from_ref, to_ref, send_sem, recv_sem, across=slice(None)):
    me, columns, per, plane, lane = here(devices)
    low = plane // 2
    target_plane = (1 - low) * (2 + place) + low * ((plane % 2 + place) % 2)
    quarter = per // 4

    def send(hop, carry):
        spot = (lane + hop) % (per // 2)
        target_lane = (1 - lanes) * (spot + spot // quarter * 2 * quarter) + lanes * (quarter + spot)
        target = target_plane * per + target_lane
        pltpu.make_async_remote_copy(
            src_ref=from_ref.at[target, :, across],
            dst_ref=to_ref.at[me, :, across],
            send_sem=send_sem,
            recv_sem=recv_sem,
            device_id=place_of(target, columns),
            device_id_type=MESH,
        ).start()
        return carry

    lax.fori_loop(0, per // 2, send, 0)


def wait_for(ref, sem, count):
    part = ref.at[pl.ds(0, count)]
    pltpu.make_async_copy(part, part, sem).wait()


def put_in_order(joined, order):
    return lax.dot_general(
        joined, order[...], (((0,), (0,)), ((), ())), preferred_element_type=jnp.float32
    ).astype(jnp.bfloat16)


def mixer_kernel(
    devices,
    tokens,
    weight,
    out_weight,
    gain_hbm,
    forward_hbm,
    first_hbm,
    turn_cos_hbm,
    turn_sin_hbm,
    usual_hbm,
    special_hbm,
    order_hbm,
    total,
    last,
    last_weight,
    early,
    order,
    gain,
    forward,
    first,
    turn_cos,
    turn_sin,
    usual,
    special,
    raw,
    held,
    held_out,
    wide,
    squares,
    sent,
    taken,
    table,
    grid,
    done,
    back,
    landed,
    ordered,
    token_sem,
    first_weight_sem,
    weight_sem,
    out_sem,
    last_sem,
    own_sem,
    send_sem,
    recv_sem,
    own_back_sem,
    back_sem,
    landed_sem,
    table_sem,
):
    me, columns, per, plane, lane = here(devices)
    pieces = token_sem.shape[0]
    rows, depth = raw.shape
    piece = rows // pieces
    first_piece = depth // pieces
    width = held.shape[2]
    units, _, slots, _ = sent.shape
    members = devices // HALVES
    near = plane // HALVES
    far = (near + 1) % HALVES
    pairs = slots // 2
    places = GROUP_WIDTH // slots
    outer = first.shape[0]
    inner = turn_cos.shape[0]
    chunks = units * HALVES
    cut_rows = rows // CUTS

    def token_copy(index):
        part = pl.ds(index * piece, piece)
        return pltpu.make_async_copy(tokens.at[part], raw.at[part], token_sem.at[index])

    def half_of(number):
        return (near + 1 + number) % HALVES

    def weight_copy(step):
        begin = pl.multiple_of((step // HALVES * HALVES + half_of(step % HALVES)) * width, width)
        return pltpu.make_async_copy(weight.at[:, pl.ds(begin, width)], held.at[step], weight_sem.at[step])

    def first_weight_copy(index):
        part = pl.ds(index * first_piece, first_piece)
        begin = pl.multiple_of(half_of(0) * width, width)
        return pltpu.make_async_copy(
            weight.at[part, pl.ds(begin, width)], held.at[0, part], first_weight_sem.at[index]
        )

    out_width = out_weight.shape[1]
    far_begin = pl.multiple_of(((units - 1) * HALVES + far) * width, width)
    out_copy = pltpu.make_async_copy(out_weight, held_out, out_sem)
    last_copy = pltpu.make_async_copy(out_weight.at[pl.ds(far_begin, width)], last_weight, last_sem)

    distant = (gain_hbm, forward_hbm, first_hbm, turn_cos_hbm, turn_sin_hbm, usual_hbm, special_hbm, order_hbm)
    nearby = (gain, forward, first, turn_cos, turn_sin, usual, special, order)
    table_copies = [
        pltpu.make_async_copy(a, b, table_sem.at[index]) for index, (a, b) in enumerate(zip(distant, nearby))
    ]
    table_copies[0].start()
    token_copy(0).start()
    arrive = greet(devices)
    for index in range(pieces):
        first_weight_copy(index).start()
    table_copies[1].start()

    block = wide.shape[0]
    table_copies[0].wait()
    wide[...] = jnp.broadcast_to(gain[...].astype(jnp.float32).reshape(1, depth), wide.shape).astype(jnp.bfloat16)

    def give_out(unit, number, part, product):
        half = half_of(number)
        scaling = jnp.concatenate([squares[part, :]] * (width // LANES), axis=1)
        hidden = (product * scaling).astype(jnp.bfloat16)
        spectrum = lax.dot_general(
            forward[...], hidden, (((1,), (1,)), ((), ())), preferred_element_type=jnp.float32
        )
        sent[unit, pl.ds(half * members, members), :, part] = spectrum.reshape(
            members, slots, part.size
        ).astype(jnp.bfloat16)

    def send_out(unit, number, part):
        for inside in range(PLANES // HALVES):
            plane_step = number * (PLANES // HALVES) + inside
            send_plane(
                devices,
                plane_step,
                sent.at[unit],
                taken.at[unit],
                send_sem.at[unit],
                recv_sem.at[unit],
                plane_step // (PLANES - 1),
                part,
            )

    def gather_squares(number, carry):
        part = pl.ds(pl.multiple_of(number * block, block), block)
        parts = [jnp.zeros((block, LANES), jnp.float32) for _ in range(4)]
        for column in range(depth // LANES):
            across = pl.ds(column * LANES, LANES)
            values = raw[part, across]
            floats = values.astype(jnp.float32)
            parts[column % 4] = parts[column % 4] + floats * floats
            raw[part, across] = values * wide[:, across]
        squares[part, :] = (parts[0] + parts[1]) + (parts[2] + parts[3])
        return carry

    stages = [(index, index + 1) for index in range(pieces)]
    for stage, (begin, end) in enumerate(stages):
        begun = (end - begin) * piece
        part = pl.ds(begin * piece, begun)
        for index in range(begin, end):
            token_copy(index).wait()
            if index == 0:
                for later in range(1, pieces):
                    token_copy(later).start()
            lax.fori_loop(index * piece // block, (index + 1) * piece // block, gather_squares, 0, unroll=2)
        mean = jnp.sum(squares[part, :], axis=-1, keepdims=True) * (1.0 / depth)
        squares[part, :] = jnp.broadcast_to(lax.rsqrt(mean + 1e-06), (begun, LANES))
        if stage == 0:
            for index in range(pieces):
                first_weight_copy(index).wait()
            table_copies[1].wait()
        if stage == len(stages) - 1:
            for step in range(1, chunks):
                weight_copy(step).start()
            for copy in table_copies[2:]:
                copy.start()
        give_out(0, 0, part, jnp.dot(raw[part, :], held[0], preferred_element_type=jnp.float32))
        if stage == 0:
            arrive()
        send_out(0, 0, part)

    everything = pl.ds(0, rows)

    def chunk(step, carry):
        unit = step // HALVES
        number = step % HALVES
        weight_copy(step).wait()
        give_out(unit, number, everything, jnp.dot(raw[...], held[step], preferred_element_type=jnp.float32))
        send_out(unit, number, everything)
        return carry

    lax.fori_loop(1, chunks, chunk, 0)
    for unit in range(units):
        pltpu.make_async_copy(sent.at[unit, me], taken.at[unit, me], own_sem.at[unit]).start()
    out_copy.start()
    last_copy.start()

    for copy in table_copies[2:]:
        copy.wait()
    zeroth_here = me % places == 0

    @pl.when(zeroth_here)
    def _():
        table[...] = special[...]

    @pl.when(jnp.logical_not(zeroth_here))
    def _():
        table[...] = usual[...]

    def turned(slot):
        a = lax.dot_general(
            grid[slot], first[...], (((0,), (0,)), ((), ())), preferred_element_type=jnp.float32
        )
        a = a[:, : 2 * outer] + a[:, 2 * outer :]
        re, im = a[:, :outer], a[:, outer:]
        c, s = turn_cos[...], turn_sin[...]
        return [(re * c + im * s).astype(jnp.bfloat16), (im * c - re * s).astype(jnp.bfloat16)]

    for unit in range(units):
        pltpu.make_async_copy(sent.at[unit, me], taken.at[unit, me], own_sem.at[unit]).wait()
        wait_for(taken.at[unit], recv_sem.at[unit], devices - 1)
        for part in range(outer // devices):
            piece_of = taken[unit, :, :, part * inner : (part + 1) * inner]
            grid[:, part * devices : (part + 1) * devices, :] = jnp.swapaxes(
                piece_of.astype(jnp.float32), 0, 1
            ).astype(jnp.bfloat16)
        for pair in range(pairs):
            b = jnp.concatenate(turned(pair) + turned(pair + pairs), axis=0)
            here_table = table if pair == 0 else usual
            o = jnp.dot(here_table[...], b, preferred_element_type=jnp.float32)
            o = o[: 2 * inner] + o[2 * inner :]
            done[pair] = o[:inner]
            done[pair + pairs] = o[inner:]
        for part in range(inner // devices):
            piece_of = done[:, part * devices : (part + 1) * devices, :]
            back[unit, :, :, part * outer : (part + 1) * outer] = jnp.swapaxes(piece_of, 0, 1).astype(jnp.bfloat16)
        last_unit = unit == units - 1
        for place, cut, lanes in itertools.product(range(2), range(CUTS if last_unit else 1), range(2)):
            send_far(
                devices,
                place,
                lanes,
                back.at[unit],
                landed.at[unit],
                back_sem.at[unit],
                landed_sem.at[unit, cut],
                pl.ds(cut * cut_rows, cut_rows) if last_unit else slice(None),
            )
        for step in range(HALVES, PLANES):
            send_plane(
                devices,
                step,
                back.at[unit],
                landed.at[unit],
                back_sem.at[unit],
                landed_sem.at[unit, CUTS],
                step // (PLANES - 1),
            )
        pltpu.make_async_copy(back.at[unit, me], landed.at[unit, me], own_back_sem.at[unit]).start()

    def joined(unit, half, across):
        parts = landed[unit, pl.ds(half * members, members), :, across].astype(jnp.float32)
        return parts.reshape(width, parts.shape[2]).astype(jnp.bfloat16)

    tile = out_width // 4
    tiles = out_width // tile
    out_copy.wait()
    for unit in range(units):
        pltpu.make_async_copy(back.at[unit, me], landed.at[unit, me], own_back_sem.at[unit]).wait()
        for number in reversed(range(HALVES)):
            half = half_of(number)
            begin = pl.multiple_of((unit * HALVES + half) * width, width)
            closing = unit == units - 1 and number == 0
            starting = unit == 0 and number == HALVES - 1
            part = pl.ds(0, cut_rows) if closing else pl.ds(0, rows)
            if closing:
                wait_for(landed.at[unit, :, :, part], landed_sem.at[unit, 0], members)
            else:
                wait_for(landed.at[unit], landed_sem.at[unit, CUTS * number], members - number)
            ordered[part, :] = put_in_order(joined(unit, half, part), order)

            def add_up(index, carry):
                across = pl.ds(pl.multiple_of(index * tile, tile), tile)
                product = jnp.dot(
                    ordered[part, :], held_out[pl.ds(begin, width), across], preferred_element_type=jnp.float32
                )
                if closing:
                    early[:, across] = (total[part, across] + product).astype(jnp.bfloat16)
                else:
                    total[:, across] = product if starting else total[:, across] + product
                return carry

            lax.fori_loop(0, tiles, add_up, 0)

    last_copy.wait()
    rest = pl.ds(cut_rows, cut_rows)
    wait_for(landed.at[units - 1, :, :, rest], landed_sem.at[units - 1, 1], members)
    last[...] = joined(units - 1, half_of(0), rest)
    for unit in range(units):
        wait_for(sent.at[unit], send_sem.at[unit], devices - 1)
        wait_for(back.at[unit], back_sem.at[unit], devices - 1)


def mixer(tokens, gain, weight, out_weight, forward, tables, order, units, devices):
    rows, depth = tokens.shape
    channels = weight.shape[1]
    slots = channels // devices // units
    outer = tables[0].shape[0]
    inner = tables[1].shape[0]
    width = channels // units // HALVES
    out_width = out_weight.shape[1]
    whole = pl.BlockSpec(memory_space=pltpu.VMEM)
    hbm = pl.BlockSpec(memory_space=pltpu.HBM)
    pieces = 4
    block = 16
    small = (gain, forward, *tables, order)
    return pl.pallas_call(
        functools.partial(mixer_kernel, devices),
        out_shape=(
            pltpu.VMEM((rows, out_width), jnp.float32),
            pltpu.VMEM((width, rows // CUTS), jnp.bfloat16),
            pltpu.VMEM((width, out_width), jnp.bfloat16),
            pltpu.VMEM((rows // CUTS, out_width), jnp.bfloat16),
            pltpu.VMEM(order.shape, order.dtype),
        ),
        in_specs=[hbm] * (3 + len(small)),
        out_specs=(whole,) * 5,
        scratch_shapes=[pltpu.VMEM(table.shape, table.dtype) for table in small[:-1]] + [
            pltpu.VMEM((rows, depth), jnp.bfloat16),
            pltpu.VMEM((units * HALVES, depth, width), jnp.bfloat16),
            pltpu.VMEM((channels, out_width), jnp.bfloat16),
            pltpu.VMEM((block, depth), jnp.bfloat16),
            pltpu.VMEM((rows, LANES), jnp.float32),
            pltpu.VMEM((units, devices, slots, rows), jnp.bfloat16),
            pltpu.VMEM((units, devices, slots, rows), jnp.bfloat16),
            pltpu.VMEM(tables[3].shape, jnp.bfloat16),
            pltpu.VMEM((slots, outer, inner), jnp.bfloat16),
            pltpu.VMEM((slots, inner, outer), jnp.float32),
            pltpu.VMEM((units, devices, slots, rows), jnp.bfloat16),
            pltpu.VMEM((units, devices, slots, rows), jnp.bfloat16),
            pltpu.VMEM((rows, width), jnp.bfloat16),
            pltpu.SemaphoreType.DMA((pieces,)),
            pltpu.SemaphoreType.DMA((pieces,)),
            pltpu.SemaphoreType.DMA((units * HALVES,)),
            pltpu.SemaphoreType.DMA,
            pltpu.SemaphoreType.DMA,
            pltpu.SemaphoreType.DMA((units,)),
            pltpu.SemaphoreType.DMA((units,)),
            pltpu.SemaphoreType.DMA((units,)),
            pltpu.SemaphoreType.DMA((units,)),
            pltpu.SemaphoreType.DMA((units,)),
            pltpu.SemaphoreType.DMA((units, CUTS + 1)),
            pltpu.SemaphoreType.DMA((len(small),)),
        ],
        compiler_params=pltpu.CompilerParams(collective_id=0, has_side_effects=True, vmem_limit_bytes=46 << 20),
    )(*[pltpu.with_memory_space_constraint(array, pltpu.HBM) for array in (tokens, weight, out_weight, *small)])


def finish_kernel(total, last, last_weight, early, order, out, staged, ordered, sems, early_sem):
    tiles = sems.shape[0]
    begin, out_width = staged.shape
    tile = out_width // tiles
    early_copy = pltpu.make_async_copy(early, out.at[pl.ds(0, begin)], early_sem)
    early_copy.start()
    ordered[...] = put_in_order(last[...], order)

    def store(index):
        across = pl.ds(index * tile, tile)
        return pltpu.make_async_copy(staged.at[:, across], out.at[pl.ds(begin, begin), across], sems.at[index])

    for index in range(tiles):
        across = pl.ds(index * tile, tile)
        product = jnp.dot(ordered[...], last_weight[:, across], preferred_element_type=jnp.float32)
        staged[:, across] = (total[pl.ds(begin, begin), across] + product).astype(jnp.bfloat16)
        store(index).start()
    early_copy.wait()
    for index in range(tiles):
        store(index).wait()


def finish(total, last, last_weight, early, order):
    rows, out_width = total.shape
    width = last_weight.shape[0]
    tiles = 4
    whole = pl.BlockSpec(memory_space=pltpu.VMEM)
    return pl.pallas_call(
        finish_kernel,
        out_shape=pltpu.HBM((rows, out_width), jnp.bfloat16),
        in_specs=[whole] * 5,
        out_specs=pl.BlockSpec(memory_space=pltpu.HBM),
        scratch_shapes=[
            pltpu.VMEM((rows // CUTS, out_width), jnp.bfloat16),
            pltpu.VMEM((rows // CUTS, width), jnp.bfloat16),
            pltpu.SemaphoreType.DMA((tiles,)),
            pltpu.SemaphoreType.DMA,
        ],
        compiler_params=pltpu.CompilerParams(vmem_limit_bytes=20 << 20),
    )(total, last, last_weight, early, order)


def local(tokens, norm_gain, in_weight, out_weight):
    rows_here = tokens.shape[0]
    channels = in_weight.shape[1]
    devices = lax.axis_size(AXES)
    slots = channels // devices
    units = max(1, slots // 16)
    length = rows_here * devices
    inner = 1 << ((length.bit_length()) // 2)
    outer = length // inner

    forward, order = channel_tables(slots // units)
    several = np.eye(channels // units // HALVES // GROUP_WIDTH)
    forward = np.kron(several, forward.astype(np.float32)).astype(jnp.bfloat16)
    order = np.kron(several, order.astype(np.float32)).T.astype(jnp.bfloat16)
    tables = position_tables(outer, inner, devices)
    parts = mixer(tokens, norm_gain, in_weight, out_weight, forward, tables, order, units, devices)
    return finish(*parts)


def solution(mesh):
    placed = (P(AXES, None), P(), P(), P())
    return jax.shard_map(
        local, mesh=mesh, in_specs=placed, out_specs=P(AXES, None), check_vma=False
    )
```
